256 devices in a mesh: sp: 64 (over z, y, core), tp: 4 (over x).
Axes of the slice: x: 4, y: 4, z: 8, core: 2. Of those that a mesh axis runs over, the one named last changes fastest.
Arguments:
- residual: bfloat16 [12288, 2048], P(('sp', 'tp')), may hold values from -6 to 6
- mixer_input: bfloat16 [12288, 512], P('sp', 'tp'), may hold values from -6 to 6
- log_gate: float32 [12288, 32], P('sp', 'tp'), may hold values from -2 to 0
- decay_rate: float32 [2, 32, 64], P(None, 'tp'), may hold values from 0 to 1
- turn_rate: float32 [2, 32, 64], P(None, 'tp'), may hold values from -1 to 1
- drive_real: float32 [2, 32, 16, 64], P(None, 'tp'), may hold values from -1 to 1
- drive_imaginary: float32 [2, 32, 16, 64], P(None, 'tp'), may hold values from -1 to 1
- read_real: float32 [2, 32, 16, 64], P(None, 'tp'), may hold values from -0.75 to 0.75
- read_imaginary: float32 [2, 32, 16, 64], P(None, 'tp'), may hold values from -0.75 to 0.75
- skip_gain: float32 [512], P('tp'), may hold values from -4 to 4
- project_weight: bfloat16 [512, 2048], replicated, may hold values from -0.25 to 0.25
- norm_gain: float32 [2048], replicated, may hold values from 0.1 to 1.9
- final_gain: float32 [2048], replicated, may hold values from 0.1 to 1.9
- routes: int32 [12288, 2], P('sp'), may hold values from 0 to 63, all different within a row; in each aligned block of 48 rows (0 to 47, 48 to 95, ...) at most 2 rows name the same one
- group_weight: float32 [12288], P('sp'), may hold values from 0.2 to 1
- expert_weight: float32 [12288, 2], P('sp'), may hold values from 0.1 to 1
- gate_weight: bfloat16 [64, 2048, 1024], P('sp', None, 'tp'), may hold values from -0.125 to 0.125
- linear_weight: bfloat16 [64, 2048, 1024], P('sp', None, 'tp'), may hold values from -0.125 to 0.125
- down_weight: bfloat16 [64, 1024, 2048], P('sp', 'tp'), may hold values from -0.1875 to 0.1875
Outputs:
- finished: bfloat16 [12288, 2048], P(('sp', 'tp'))
The draws below stay inside these ranges and needn't reach their ends.
Inputs may be any that keep to these rules, and one draw needn't show every extreme that they name: `routes`: each row names 2 different experts. In each aligned block of 48 rows no expert is named by more than 2 rows; some expert is named by exactly 2 rows of some block.
All inputs are finite; a program needn't handle non-finite values.
Results may differ from the reference program's by a relative error of at most 0.006.
Values may be sent and summed in bfloat16 or wider, within the bound.
No kernel may reach another device: no remote copies, remote signals or barrier semaphores. Data moves between devices by JAX's collectives and lax.ppermute only.
A program may use at most 128 MiB of HBM per device.

```python
import math
import jax
import jax.numpy as jnp
import numpy as np
from jax import lax

D = 2048
S_GROUPS = 32
GROUP_DIM = 16
S_STATE = 64
S_WIDTH = 512
D_EXPERT = 1024
TOP_K = 2
TOK_DEV = 192
TOKENS = 12288
TOK_SHARE = 48
EXPERTS = 64
SLOTS = 2
N_SP = 64
N_TP = 4


def draw_decay_rate(key, part):
    pick_key, fast_key, slow_key = jax.random.split(key, 3)
    fast_share = 0.5
    is_fast = jax.random.uniform(pick_key, (2, S_GROUPS, 1)) < fast_share
    fast_rate = jnp.exp(jax.random.uniform(fast_key, (2, S_GROUPS, S_STATE), minval=jnp.log(0.01), maxval=jnp.log(1.0 / 30.0)))
    slow_rate = jnp.exp(jax.random.uniform(slow_key, (2, S_GROUPS, S_STATE), minval=jnp.log(0.05), maxval=jnp.log(0.3))) / TOKENS
    return jnp.where(is_fast, fast_rate, slow_rate).astype(jnp.float32)


def draw_log_gate(key, part):
    factor_key, rough_key, place_key, drop_key = jax.random.split(key, 4)
    blocks = TOKENS // TOK_DEV
    factor = jnp.exp(jax.random.uniform(factor_key, (blocks, 1, S_GROUPS), minval=0.0, maxval=jnp.log(4.0)))
    roughness = jnp.exp(0.5 * jnp.clip(jax.random.normal(rough_key, (blocks, TOK_DEV, S_GROUPS)), -3.0, 3.0))
    steady = -0.2 / TOKENS * (factor * roughness).reshape(TOKENS, S_GROUPS)
    places = jax.random.randint(place_key, (2,), 0, TOKENS)
    drop_sizes = jnp.log(jax.random.uniform(drop_key, (2, S_GROUPS), minval=0.5, maxval=0.8))
    matches = (jnp.arange(TOKENS, dtype=jnp.int32)[:, None] == places[None, :]).astype(jnp.float32)
    return (steady + jnp.dot(matches, drop_sizes, precision=lax.Precision.HIGHEST)).astype(jnp.float32)


def shard_levels(stream_key, shape, pieces, smallest, high):
    def one(axis_at, shards_of):
        draws = jax.random.uniform(jax.random.fold_in(jax.random.fold_in(stream_key, 6), axis_at), (shards_of,), jnp.float32, smallest / len(pieces), high / len(pieces))
        return jnp.repeat(jnp.exp(draws), shape[axis_at] // shards_of).reshape((-1,) + (1,) * (len(shape) - axis_at - 1))

    level = one(*pieces[0])
    for cut in pieces[1:]:
        level = level * one(*cut)
    return level


def assign_block(rng, own, number, rows, number_of, top, most, skew):
    ranking = jax.random.permutation(rng, number_of)
    heavy_load, common = shares(number_of, rows * top, most, skew, True), shares(number_of, rows * top, most, skew, False)
    places = jnp.arange(number_of)

    def named(tallies, turn):
        used = int((tallies > 0).sum())
        fixed = max(1, used // 4)
        passed = fixed + (places - fixed + turn * (used - fixed)) % max(1, number_of - fixed)
        return jnp.zeros((number_of,), jnp.int32).at[ranking[jnp.where(places < fixed, places, passed)]].set(jnp.asarray(tallies, jnp.int32))

    tallies = jnp.where(number % 4 == 0, named(heavy_load, number // 4), named(common, number - number // 4 - 1))
    mixed = jax.random.permutation(jax.random.fold_in(own, 3), number_of)
    source_of, taker = mixed[0:number_of // 2 * 2:2], mixed[1:number_of // 2 * 2:2]
    room = jnp.minimum(tallies[source_of] - 1, most - tallies[taker]) // 2
    room = jnp.where((source_of == ranking[0]) | (taker == ranking[0]) | (tallies[taker] == 0), 0, jnp.maximum(room, 0))
    passed = jax.random.randint(jax.random.fold_in(own, 4), (number_of // 2,), 0, 1 << 20) % (room + 1)
    tallies = tallies.at[source_of].add(-passed).at[taker].add(passed)
    labels = jnp.searchsorted(jnp.cumsum(tallies), jnp.arange(rows * top), side="right").astype(jnp.int32)
    table = labels.reshape(top, rows).T
    table = table[jax.random.permutation(jax.random.fold_in(own, 1), rows)]
    turn = jax.random.randint(jax.random.fold_in(own, 2), (rows, 1), 0, top)
    return jnp.take_along_axis(table, (jnp.arange(top)[None, :] + turn) % top, axis=1)


def shares(count, total, limit, slope, full):
    weights = [(1 << 20) // math.isqrt(grade ** slope) + 1 for grade in range(1, count + 1)]
    largest = limit if full else min(limit, max(-(-total // count), total * weights[0] // sum(weights)))
    least = 1 if total - largest >= count - 1 else 0
    given, surplus = [largest] + [least] * (count - 1), total - largest - least * (count - 1)
    while surplus > 0:
        candidates = [i for i in range(1, count) if given[i] < largest] or [i for i in range(1, count) if given[i] < limit]
        pool, budget = sum([weights[i] for i in candidates]), surplus
        for i in candidates:
            extra = min(limit - given[i], max(1, budget * weights[i] // pool), surplus)
            given[i] = given[i] + extra
            surplus = surplus - extra
    return np.array(given)


def centred(key, extent, width, most, cuts=(), kind=jnp.bfloat16):
    drawn = width * jax.random.normal(key, extent, jnp.float32)
    if cuts:
        drawn = drawn * shard_levels(key, extent, cuts, -0.22, 0.18)
    return jnp.clip(drawn, -most, most).astype(kind)


def setup_inputs(seed: int = 0) -> dict:
    key_list = jax.random.split(jax.random.key(seed), 20)
    residual = centred(key_list[0], (TOKENS, D), 1.0, 6.0, ((0, 256),))
    mixer_input = centred(key_list[1], (TOKENS, S_WIDTH), 1.0, 6.0, ((0, 64), (1, 4)))
    log_gate = draw_log_gate(jax.random.fold_in(key_list[19], 71), 0)
    decay_rate = draw_decay_rate(jax.random.fold_in(key_list[19], 71), 0)
    turn_rate = jnp.clip(jax.random.uniform(key_list[4], (2, S_GROUPS, S_STATE), jnp.float32, -1.0, 1.0) * shard_levels(key_list[4], (2, S_GROUPS, S_STATE), ((1, 4),), -0.4, 0.0), -1.0, 1.0)
    drive_real = centred(key_list[5], (2, S_GROUPS, GROUP_DIM, S_STATE), (2 * GROUP_DIM) ** -0.5, 1.0, ((1, 4),), jnp.float32)
    drive_imaginary = centred(key_list[6], (2, S_GROUPS, GROUP_DIM, S_STATE), (2 * GROUP_DIM) ** -0.5, 1.0, ((1, 4),), jnp.float32)
    read_real = centred(key_list[7], (2, S_GROUPS, GROUP_DIM, S_STATE), S_STATE ** -0.5, 0.75, ((1, 4),), jnp.float32)
    read_imaginary = centred(key_list[8], (2, S_GROUPS, GROUP_DIM, S_STATE), S_STATE ** -0.5, 0.75, ((1, 4),), jnp.float32)
    skip_gain = centred(key_list[9], (S_WIDTH,), 1.0, 4.0, ((0, 4),), jnp.float32)
    project_weight = centred(key_list[10], (S_WIDTH, D), S_WIDTH ** -0.5, 0.25)
    norm_gain = jnp.clip(1.0 + 0.18 * jax.random.normal(key_list[11], (D,), jnp.float32), 0.1, 1.9)
    final_gain = jnp.clip(1.0 + 0.18 * jax.random.normal(key_list[12], (D,), jnp.float32), 0.1, 1.9)
    routes_keys = jax.random.split(jax.random.fold_in(key_list[13], 1), TOKENS // TOK_SHARE)
    routes_turns = jax.random.permutation(jax.random.fold_in(key_list[13], 3), TOKENS // TOK_SHARE)
    routes = jax.vmap(lambda own, number: assign_block(jax.random.fold_in(key_list[13], 2), own, number, TOK_SHARE, EXPERTS, TOP_K, SLOTS, 2))(routes_keys, routes_turns).reshape((TOKENS, TOP_K))
    group_weight = jnp.clip(jnp.exp(math.log(1.0) - 1.609438 * jax.random.uniform(key_list[14], (TOKENS,), jnp.float32) ** shard_levels(key_list[14], (TOKENS,), ((0, 64),), -0.2, 0.2)), 0.2, 1.0)
    expert_weight = jnp.clip(jnp.exp(math.log(1.0) - 2.3025851 * jax.random.uniform(key_list[15], (TOKENS, TOP_K), jnp.float32) ** shard_levels(key_list[15], (TOKENS, TOP_K), ((0, 64),), -0.2, 0.2)), 0.1, 1.0)
    gate_weight = centred(key_list[16], (EXPERTS, D, D_EXPERT), D ** -0.5, 0.125, ((0, 64), (2, 4)))
    linear_weight = centred(key_list[17], (EXPERTS, D, D_EXPERT), D ** -0.5, 0.125, ((0, 64), (2, 4)))
    down_weight = centred(key_list[18], (EXPERTS, D_EXPERT, D), D_EXPERT ** -0.5, 0.1875, ((0, 64), (1, 4)))
    return {"residual": residual, "mixer_input": mixer_input, "log_gate": log_gate, "decay_rate": decay_rate, "turn_rate": turn_rate, "drive_real": drive_real, "drive_imaginary": drive_imaginary, "read_real": read_real, "read_imaginary": read_imaginary, "skip_gain": skip_gain, "project_weight": project_weight, "norm_gain": norm_gain, "final_gain": final_gain, "routes": routes, "group_weight": group_weight, "expert_weight": expert_weight, "gate_weight": gate_weight, "linear_weight": linear_weight, "down_weight": down_weight}


deep_alpha = 2.0 ** 0.25
norm_epsilon = 1e-05
highest = lax.Precision.HIGHEST

def layer_norm(values, gain):
    center = values - lax.optimization_barrier(jnp.mean(values, axis=-1, keepdims=True))
    spread = lax.optimization_barrier(jnp.mean(center * center, axis=-1, keepdims=True))
    return center * lax.rsqrt(spread + norm_epsilon) * gain

def sweep(inputs, log_gate, rate_row, turn_row, drive_real, drive_imaginary, read_real, read_imaginary, backward):
    input_scale = jnp.sqrt(1.0 - jnp.exp(-2.0 * rate_row))
    retain = jnp.exp(-rate_row)
    step_real = retain * jnp.cos(turn_row)
    step_imaginary = retain * jnp.sin(turn_row)

    def advance(carried, current):
        state_real, state_imaginary = carried
        token_row, gate_row = current
        push_real = jnp.einsum('gh,ghp->gp', token_row, drive_real, precision=highest) * input_scale
        push_imaginary = jnp.einsum('gh,ghp->gp', token_row, drive_imaginary, precision=highest) * input_scale
        factor = jnp.exp(gate_row)[:, None]
        new_real = factor * (step_real * state_real - step_imaginary * state_imaginary) + push_real
        new_imaginary = factor * (step_real * state_imaginary + step_imaginary * state_real) + push_imaginary
        output = jnp.einsum('gp,ghp->gh', new_real, read_real, precision=highest) - jnp.einsum('gp,ghp->gh', new_imaginary, read_imaginary, precision=highest)
        return ((new_real, new_imaginary), output)
    initial = jnp.zeros(rate_row.shape, jnp.float32)
    _, outputs = lax.scan(advance, (initial, initial), (inputs, log_gate), reverse=backward)
    return outputs

def reference(residual, mixer_input, log_gate, decay_rate, turn_rate, drive_real, drive_imaginary, read_real, read_imaginary, skip_gain, project_weight, norm_gain, final_gain, routes, group_weight, expert_weight, gate_weight, linear_weight, down_weight):
    inputs = mixer_input.astype(jnp.float32).reshape(TOKENS, S_GROUPS, GROUP_DIM)
    readout = sweep(inputs, log_gate, decay_rate[0], turn_rate[0], drive_real[0], drive_imaginary[0], read_real[0], read_imaginary[0], False)
    readout = readout + sweep(inputs, log_gate, decay_rate[1], turn_rate[1], drive_real[1], drive_imaginary[1], read_real[1], read_imaginary[1], True)
    readout = readout + skip_gain.reshape(S_GROUPS, GROUP_DIM) * inputs
    activated = jax.nn.gelu(readout).reshape(TOKENS, S_WIDTH).astype(jnp.bfloat16)
    branch = jnp.dot(activated, project_weight, preferred_element_type=jnp.float32)
    middle = layer_norm(deep_alpha * residual.astype(jnp.float32) + branch, norm_gain)
    middle_rows = middle.astype(jnp.bfloat16)
    flat_experts = routes.reshape(-1)
    sorted_order = jnp.argsort(flat_experts, stable=True).astype(jnp.int32)
    counts = lax.optimization_barrier(jnp.sum((flat_experts[:, None] == jnp.arange(EXPERTS, dtype=jnp.int32)[None, :]).astype(jnp.int32), axis=0))
    starts = (jnp.cumsum(counts) - counts).astype(jnp.int32)
    capacity = N_SP * N_TP * SLOTS
    assigned = TOKENS * TOP_K
    piece_width = D_EXPERT // N_TP

    def run_expert(expert):
        offsets = jnp.arange(capacity, dtype=jnp.int32)
        is_valid = offsets < counts[expert]
        chosen = sorted_order[jnp.minimum(starts[expert] + offsets, assigned - 1)]
        row_inputs = middle_rows[chosen // TOP_K]
        gate_part = jnp.dot(row_inputs, gate_weight[expert], preferred_element_type=jnp.float32)
        linear_part = jnp.dot(row_inputs, linear_weight[expert], preferred_element_type=jnp.float32)
        hidden = (jax.nn.silu(gate_part) * linear_part).astype(jnp.bfloat16)
        running = jnp.zeros((capacity, D), jnp.float32)
        for member in range(N_TP):
            partial_value = jnp.dot(hidden[:, member * piece_width:(member + 1) * piece_width], down_weight[expert, member * piece_width:(member + 1) * piece_width], preferred_element_type=jnp.float32)
            rounded = lax.optimization_barrier(partial_value.astype(jnp.bfloat16))
            running = running + rounded.astype(jnp.float32)
        return (running.astype(jnp.bfloat16), jnp.where(is_valid, chosen, assigned).astype(jnp.int32))
    results, targets = lax.map(run_expert, jnp.arange(EXPERTS, dtype=jnp.int32))
    answers = jnp.zeros((assigned, D), jnp.bfloat16).at[targets.reshape(-1)].set(results.reshape(-1, D), mode='drop')
    mixing = group_weight[:, None] * expert_weight / lax.optimization_barrier(jnp.sum(expert_weight, axis=1, keepdims=True))
    routed = lax.optimization_barrier(jnp.sum(mixing[:, :, None] * answers.reshape(TOKENS, TOP_K, D).astype(jnp.float32), axis=1))
    finished = layer_norm(deep_alpha * middle + routed, final_gain)
    return finished.astype(jnp.bfloat16)
```

```python
import jax
import jax.numpy as jnp
from jax import lax
from jax.experimental import pallas as pl
from jax.experimental.pallas import tpu as pltpu
from jax.sharding import PartitionSpec as P


deep_alpha = 2.0**0.25
norm_epsilon = 1e-05
f32 = jnp.float32
bf16 = jnp.bfloat16
VMEM = pltpu.MemorySpace.VMEM
lanes = 128
gate_row = 8
sent_rows = 9


def iota(shape, dim):
    return lax.broadcasted_iota(jnp.int32, shape, dim)


def mm(a, b):
    return lax.dot_general(a, b, (((1,), (0,)), ((), ())), preferred_element_type=f32)


def mm_nt(a, b):
    return lax.dot_general(a, b, (((1,), (1,)), ((), ())), preferred_element_type=f32)


def mm_tn(a, b):
    return lax.dot_general(a, b, (((0,), (0,)), ((), ())), preferred_element_type=f32)


def split(value, pieces):
    found = []
    for _ in range(pieces - 1):
        high = value.astype(bf16)
        found.append(high)
        value = value - high.astype(f32)
    return found + [value.astype(bf16)]


def exact_left(table, value):
    total = None
    for piece in split(value, 3):
        part = mm(table, piece)
        total = part if total is None else total + part
    return total


def exact_right(value, table):
    total = None
    for piece in split(value, 3):
        part = mm(piece, table)
        total = part if total is None else total + part
    return total


def reversal(size):
    return (iota((size, size), 0) + iota((size, size), 1) == size - 1).astype(f32).astype(bf16)


def as_row(table, groups, states):
    wide = jnp.concatenate([table] * groups, axis=1)
    keep = iota(wide.shape, 0) == iota(wide.shape, 1) // states
    return jnp.sum(jnp.where(keep, wide, 0.0), axis=0, keepdims=True)


def block_diagonal(table, groups, states):
    each = table.shape[0] // groups
    wide = jnp.concatenate([table] * groups, axis=1)
    keep = iota(wide.shape, 0) // each == iota(wide.shape, 1) // states
    return jnp.where(keep, wide, 0.0)


def steps_of(rate, turn, groups, states):
    retain = jnp.exp(-rate)
    return (
        as_row(retain * jnp.cos(turn), groups, states),
        as_row(retain * jnp.sin(turn), groups, states),
    )


def cmul(a, b):
    return (a[0] * b[0] - a[1] * b[1], a[0] * b[1] + a[1] * b[0])


def local_kernel(
    x_ref, gate_ref, rate_ref, turn_ref, drive_re_ref, drive_im_ref,
    send_ref, state_re_ref, state_im_ref, wide_ref, step_ref,
):
    length = x_ref.shape[0]
    groups, states = rate_ref.shape[1:]
    width = groups * states
    tiles = width // lanes
    turned = reversal(length)
    x = x_ref[...]
    log_gate = gate_ref[...]
    spread = (iota((groups, width), 0) == iota((groups, width), 1) // states).astype(f32).astype(bf16)
    factors = split(jnp.exp(log_gate), 3)
    for k in range(2):
        rate = rate_ref[k]
        step_re, step_im = steps_of(rate, turn_ref[k], groups, states)
        scale = as_row(jnp.sqrt(1.0 - jnp.exp(-2.0 * rate)), groups, states)
        x_k = x if k == 0 else mm(turned, x).astype(bf16)
        x_two = jnp.concatenate([x_k, x_k], axis=1)
        gates = None
        for piece in factors:
            piece_k = piece if k == 0 else mm(piece, turned).astype(bf16)
            part = mm_tn(piece_k, spread)
            gates = part if gates is None else gates + part
        pushes = []
        for drive_ref in (drive_re_ref, drive_im_ref):
            table = block_diagonal(drive_ref[k], groups, states) * scale
            pushes.append(mm(x_two, jnp.concatenate(split(table, 2), axis=0)))
        for j in range(tiles):
            cols = slice(j * lanes, (j + 1) * lanes)
            rows = pl.ds(k * tiles + j, length, stride=2 * tiles)
            wide_ref[rows, :] = gates[:, cols]
            state_re_ref[rows, :] = pushes[0][:, cols]
            state_im_ref[rows, :] = pushes[1][:, cols]
            at = k * tiles + j
            step_ref[at : at + 1, :] = step_re[:, cols]
            step_ref[2 * tiles + at : 2 * tiles + at + 1, :] = step_im[:, cols]
    high = 2 * tiles
    w_re = step_ref[0:high, :]
    w_im = step_ref[high : 2 * high, :]

    def advance(t, carried):
        re, im = carried
        at = pl.ds(pl.multiple_of(t * high, high), high)
        factor = wide_ref[at, :]
        a_re, a_im = factor * w_re, factor * w_im
        new_re = (state_re_ref[at, :] + a_re * re) - a_im * im
        new_im = (state_im_ref[at, :] + a_re * im) + a_im * re
        state_re_ref[at, :] = new_re
        state_im_ref[at, :] = new_im
        return new_re, new_im

    zero = jnp.zeros((high, lanes), f32)
    re, im = lax.fori_loop(0, length, advance, (zero, zero), unroll=8)
    step_ref[0:high, :] = re
    step_ref[high : 2 * high, :] = im
    blocks = send_ref.shape[0] // sent_rows
    later = iota((blocks, lanes), 0) > lax.axis_index("sp")
    for part in range(2):
        for j in range(tiles):
            forward = step_ref[part * high + j : part * high + j + 1, :]
            backward = step_ref[part * high + tiles + j : part * high + tiles + j + 1, :]
            send_ref[pl.ds(part * tiles + j, blocks, stride=sent_rows), :] = jnp.where(
                later, forward, backward
            )
    total = jnp.sum(log_gate, axis=1, keepdims=True)
    thin = iota((groups, lanes), 0) == iota((groups, lanes), 1) // (lanes // groups)
    total_row = jnp.sum(jnp.where(thin, total, 0.0), axis=0, keepdims=True)
    send_ref[pl.ds(gate_row, blocks, stride=sent_rows), :] = jnp.broadcast_to(
        total_row, (blocks, lanes)
    )


def powers(step, length, backward):
    width = step[0].shape[1]
    exponent = iota((8, width), 0)
    exponent = 8 - exponent if backward else exponent + 1
    current = step
    rows = (jnp.ones((8, width), f32), jnp.zeros((8, width), f32))
    for bit in range(4):
        taken = (exponent >> bit) % 2 == 1
        more = cmul(rows, current)
        rows = tuple(jnp.where(taken, m, r) for m, r in zip(more, rows))
        if bit < 3:
            current = cmul(current, current)
    grown = {8: (rows, current)}
    size = 8
    while size * 2 <= length:
        rows, current = grown[size]
        more = cmul(rows, current)
        pair = (more, rows) if backward else (rows, more)
        rows = tuple(jnp.concatenate([a, b], axis=0) for a, b in zip(*pair))
        grown[size * 2] = (rows, cmul(current, current))
        size *= 2
    rows, current = grown[size]
    rest = length - size
    if rest:
        tail_rows, tail_power = grown[rest]
        more = cmul(tail_rows, current)
        pair = (more, rows) if backward else (rows, more)
        rows = tuple(jnp.concatenate([a, b], axis=0) for a, b in zip(*pair))
        current = cmul(current, tail_power)
    return rows, current


def powers_at(step, exponents, most):
    rows = (jnp.ones(exponents.shape, f32), jnp.zeros(exponents.shape, f32))
    bit = 0
    while (1 << bit) <= most:
        taken = (exponents >> bit) % 2 == 1
        more = cmul(rows, step)
        rows = tuple(jnp.where(taken, m, r) for m, r in zip(more, rows))
        step = cmul(step, step)
        bit += 1
    return rows


def beside_kernel(
    x_ref, gate_ref, rate_ref, turn_ref, read_re_ref, read_im_ref, skip_ref,
    state_re_ref, state_im_ref, routes_ref, group_ref, weight_ref,
    local_ref, run_ref, chain_ref, pick_ref, mix_ref,
):
    length = x_ref.shape[0]
    groups, states = rate_ref.shape[1:]
    width = groups * states
    tiles = width // lanes
    each = lanes // groups
    blocks = chain_ref.shape[1]
    here = lax.axis_index("sp")
    thin = (iota((groups, lanes), 0) == iota((groups, lanes), 1) // each).astype(f32).astype(bf16)
    log_gate = gate_ref[...]
    rows, cols = iota((length, length), 0), iota((length, length), 1)
    outs = []
    for k in range(2):
        total = None
        for part, state_ref in enumerate((state_re_ref, state_im_ref)):
            read_ref = (read_re_ref, read_im_ref)[part]
            table_high, table_low = split(block_diagonal(read_ref[k], groups, states), 2)
            for j in range(tiles):
                state = state_ref[pl.ds(k * tiles + j, length, stride=2 * tiles), :]
                state_high, state_low = split(state, 2)
                lane = slice(j * lanes, (j + 1) * lanes)
                value = (
                    mm_nt(state_high, table_high[:, lane])
                    + mm_nt(state_low, table_high[:, lane])
                    + mm_nt(state_high, table_low[:, lane])
                )
                if part:
                    value = -value
                total = value if total is None else total + value
        outs.append(total)
        seen = (rows <= cols) if k == 0 else (rows >= cols)
        run = jnp.exp(exact_right(log_gate, seen.astype(f32).astype(bf16)))
        spread = None
        for piece in split(run, 3):
            more = mm_tn(piece, thin)
            spread = more if spread is None else spread + more
        run_ref[k] = spread
        step = steps_of(rate_ref[k], turn_ref[k], groups, states)
        whole = powers_at(step, jnp.full((1, width), length, jnp.int32), length)
        source = iota((blocks, width), 0)
        gap = here - 1 - source if k == 0 else source - 1 - here
        chained = powers_at(whole, jnp.maximum(gap, 0), blocks - 1)
        for part in range(2):
            chain_ref[2 * k + part] = jnp.where(gap >= 0, chained[part], 0.0)
    local_ref[...] = (
        outs[0] + exact_left(reversal(length), outs[1]) + skip_ref[...] * x_ref[...].astype(f32)
    )
    slots, share = pick_ref.shape
    routes = routes_ref[...]
    weights = weight_ref[...]
    scaled = group_ref[...] * weights / (weights[0:1] + weights[1:2])
    place = iota((slots, length), 0)
    first = routes[0:1] == place // 2
    second = routes[1:2] == place // 2
    named = jnp.where(first | second, 1.0, 0.0)
    before = (rows < cols) & (rows // share == cols // share)
    prior = mm(named.astype(bf16), before.astype(f32).astype(bf16))
    picked = jnp.where(prior == (place % 2).astype(f32), named, 0.0)
    base = lax.axis_index("tp") * share
    own = (iota((length, share), 0) == base + iota((length, share), 1)).astype(f32).astype(bf16)
    pick_ref[...] = mm(picked.astype(bf16), own).astype(bf16)
    own = (iota((share, length), 1) == base + iota((share, length), 0)).astype(f32).astype(bf16)
    mixing = None
    for piece in split(picked * jnp.where(first, scaled[0:1], scaled[1:2]), 3):
        more = mm_nt(own, piece)
        mixing = more if mixing is None else mixing + more
    mix_ref[...] = mixing


def carry_kernel(
    come_ref, local_ref, run_ref, chain_ref, rate_ref, turn_ref, read_re_ref, read_im_ref,
    own_ref, next_ref, last_ref, far_ref, act_ref,
):
    here, member = lax.axis_index("sp"), lax.axis_index("tp")
    blocks, width = chain_ref.shape[1:]
    groups, states = rate_ref.shape[1:]
    tiles = width // lanes
    length = local_ref.shape[0]
    came = [
        jnp.concatenate(
            [come_ref[pl.ds(p * tiles + j, blocks, stride=sent_rows), :] for j in range(tiles)],
            axis=1,
        )
        for p in range(2)
    ]
    logs = come_ref[pl.ds(gate_row, blocks, stride=sent_rows), :]
    each = lanes // groups
    fan = (iota((lanes, width), 0) == each * (iota((lanes, width), 1) // states)).astype(f32)
    fan = fan.astype(bf16)
    source, mid = iota((blocks, blocks), 0), iota((blocks, blocks), 1)
    total = local_ref[...]
    for k in range(2):
        if k == 0:
            between = (mid > source) & (mid < here)
        else:
            between = (mid < source) & (mid > here)
        fade = jnp.exp(exact_left(between.astype(f32).astype(bf16), logs))
        fade = exact_right(fade, fan)
        chain = (chain_ref[2 * k] * fade, chain_ref[2 * k + 1] * fade)
        carry = [jnp.sum(v, axis=0, keepdims=True) for v in cmul(chain, came)]
        real = block_diagonal(read_re_ref[k], groups, states)
        imaginary = block_diagonal(read_im_ref[k], groups, states)
        step = steps_of(rate_ref[k], turn_ref[k], groups, states)
        grown, _ = powers(step, length, k == 1)
        first = carry[0] * real - carry[1] * imaginary
        second = -(carry[0] * imaginary + carry[1] * real)
        value = None
        for part, side in enumerate((first, second)):
            side_high, side_low = split(side, 2)
            high, low = split(grown[part], 2)
            more = mm_nt(high, side_high) + mm_nt(low, side_high) + mm_nt(high, side_low)
            value = more if value is None else value + more
        total = total + run_ref[k] * value
    act_ref[...] = jax.nn.gelu(total).astype(bf16)
    share = own_ref.shape[0]
    members = act_ref.shape[0] // share
    for shift, out_ref in enumerate((own_ref, next_ref, far_ref, last_ref)):
        at = lax.rem(member + shift, members) * share
        out_ref[...] = act_ref[pl.ds(pl.multiple_of(at, share), share), :]


def normed(values, gain):
    center = values - jnp.mean(values, axis=-1, keepdims=True)
    spread = jnp.mean(center * center, axis=-1, keepdims=True)
    return center * lax.rsqrt(spread + norm_epsilon) * gain


def to_lines(rows, rows_ref, out_ref):
    count, width = rows.shape
    each = width // lanes
    for q in range(each):
        rows_ref[pl.ds(q, count, stride=each), :] = rows[:, q * lanes : (q + 1) * lanes]
    out_ref[...] = rows_ref[...].astype(bf16)


def from_lines(lines_ref, rows_ref, each):
    count = lines_ref.shape[0] // each
    rows_ref[...] = lines_ref[...].astype(f32)
    return [rows_ref[pl.ds(q, count, stride=each), :].astype(bf16) for q in range(each)]


def branch_kernel(
    weight_hbm, residual_hbm, own_ref, from_last_ref, from_far_ref, from_next_ref, gain_ref,
    pick_ref, middle_ref, out_ref, rows_ref, weight_ref, residual_ref, sems,
):
    member = lax.axis_index("tp")
    channels = own_ref.shape[1]
    members = weight_ref.shape[0] // channels
    copies = []
    for shift in range(members):
        at = lax.rem(member + shift, members) * channels
        rows = pl.ds(pl.multiple_of(at, channels), channels)
        here = pl.ds(shift * channels, channels)
        copies.append(
            pltpu.make_async_copy(weight_hbm.at[rows, :], weight_ref.at[here, :], sems.at[shift])
        )
    copies.append(pltpu.make_async_copy(residual_hbm, residual_ref, sems.at[members]))
    for copy in copies:
        copy.start()
    branch = None
    for shift, part_ref in enumerate((own_ref, from_next_ref, from_far_ref, from_last_ref)):
        copies[shift].wait()
        more = mm(part_ref[...], weight_ref[shift * channels : (shift + 1) * channels, :])
        branch = more if branch is None else branch + more
    copies[members].wait()
    middle = normed(deep_alpha * residual_ref[...].astype(f32) + branch, gain_ref[...])
    middle_ref[...] = middle
    to_lines(mm(pick_ref[...], middle.astype(bf16)), rows_ref, out_ref)


def hidden_kernel(top_ref, low_ref, gate_ref, linear_ref, out_ref, rows_ref):
    each = gate_ref.shape[0] // lanes
    half = top_ref.shape[0] // each
    for at, ref in ((0, top_ref), (half, low_ref)):
        rows = jnp.concatenate(from_lines(ref, rows_ref, each), axis=1)
        gate = mm(rows, gate_ref[...])
        linear = mm(rows, linear_ref[...])
        out_ref[at : at + half, :] = (jax.nn.silu(gate) * linear).astype(bf16)


def down_kernel(own_ref, last_ref, next_ref, w_own_ref, w_last_ref, w_next_ref, out_ref):
    total = mm(own_ref[...], w_own_ref[...]).astype(bf16).astype(f32)
    total = total + mm(last_ref[...], w_last_ref[...]).astype(bf16).astype(f32)
    out_ref[...] = total + mm(next_ref[...], w_next_ref[...]).astype(bf16).astype(f32)


def answer_kernel(sum_ref, far_ref, w_far_top_ref, w_far_low_ref, out_ref, rows_ref):
    half = w_far_top_ref.shape[0]
    far = mm(far_ref[:, :half], w_far_top_ref[...]) + mm(far_ref[:, half:], w_far_low_ref[...])
    to_lines(sum_ref[...] + far.astype(bf16).astype(f32), rows_ref, out_ref)


def final_kernel(answers_ref, mix_ref, middle_ref, gain_ref, out_ref, rows_ref):
    each = middle_ref.shape[1] // lanes
    mixing = split(mix_ref[...], 3)
    routed = []
    for answers in from_lines(answers_ref, rows_ref, each):
        routed.append(mm(mixing[0], answers) + mm(mixing[1], answers) + mm(mixing[2], answers))
    routed = jnp.concatenate(routed, axis=1)
    out_ref[...] = normed(deep_alpha * middle_ref[...] + routed, gain_ref[...]).astype(bf16)


def shape(dims, dtype):
    return jax.ShapeDtypeStruct(dims, dtype)


def call(kernel, outs, scratch, cost, *args, room=16, kept=0):
    many = isinstance(outs, (list, tuple))
    whole = pl.BlockSpec(memory_space=VMEM)
    return pl.pallas_call(
        kernel,
        out_shape=outs,
        in_specs=[pl.BlockSpec(memory_space=pl.ANY)] * kept + [whole] * (len(args) - kept),
        out_specs=[whole] * len(outs) if many else whole,
        scratch_shapes=scratch,
        compiler_params=pltpu.CompilerParams(vmem_limit_bytes=room << 20),
        cost_estimate=pl.CostEstimate(flops=cost, bytes_accessed=1 << 20, transcendentals=0),
    )(*args)


def on_device(
    residual, mixer_input, log_gate, decay_rate, turn_rate, drive_real, drive_imaginary,
    read_real, read_imaginary, skip_gain, project_weight, norm_gain, final_gain, routes,
    group_weight, expert_weight, gate_weight, linear_weight, down_weight,
):
    length, channels = mixer_input.shape
    groups, states = decay_rate.shape[1:]
    width = groups * states
    share, model = residual.shape
    blocks = lax.axis_size("sp")
    members = lax.axis_size("tp")
    slots = 2 * blocks
    right = [(i, (i + 1) % members) for i in range(members)]
    left = [(i, (i - 1) % members) for i in range(members)]
    across = [(i, (i + 2) % members) for i in range(members)]

    def moved(array, way):
        return lax.ppermute(array, "tp", way)

    down = down_weight[0]
    half_down = down.shape[0] // 2
    down_last = moved(down, right)
    down_next = moved(down, left)

    flat = lambda table: table.reshape(2, -1, states)
    send, state_re, state_im = call(
        local_kernel,
        [
            shape((blocks * sent_rows, lanes), f32),
            shape((length * 2 * width // lanes, lanes), f32),
            shape((length * 2 * width // lanes, lanes), f32),
        ],
        [
            pltpu.VMEM((length * 2 * width // lanes, lanes), f32),
            pltpu.VMEM((4 * width // lanes, lanes), f32),
        ],
        1 << 30,
        mixer_input, log_gate.T, decay_rate, turn_rate, flat(drive_real), flat(drive_imaginary),
        room=60,
    )
    come = lax.all_to_all(
        send.reshape(blocks, 1, sent_rows * lanes), "sp", split_axis=0, concat_axis=0,
        tiled=True,
    ).reshape(blocks * sent_rows, lanes)
    local, run, chain, pick, mix = call(
        beside_kernel,
        [
            shape((length, lanes), f32),
            shape((2, length, lanes), f32),
            shape((4, blocks, width), f32),
            shape((slots, share), bf16),
            shape((share, slots), f32),
        ],
        [],
        1 << 30,
        mixer_input, log_gate.T, decay_rate, turn_rate, flat(read_real), flat(read_imaginary),
        skip_gain[None], state_re, state_im, routes.T, group_weight[None], expert_weight.T,
        room=60,
    )
    own, to_next, to_last, to_far = call(
        carry_kernel,
        [shape((share, channels), bf16)] * 4,
        [pltpu.VMEM((length, channels), bf16)],
        1 << 29,
        come, local, run, chain, decay_rate, turn_rate, flat(read_real), flat(read_imaginary),
        room=60,
    )
    from_last = moved(to_next, right)
    from_far = moved(to_far, across)
    from_next = moved(to_last, left)
    down_far_top = moved(down_last[:half_down], right)
    down_far_low = moved(down_next[half_down:], left)
    lines = slots * model // lanes
    middle, outgoing = call(
        branch_kernel,
        [shape((share, model), f32), shape((lines, lanes), bf16)],
        [
            pltpu.VMEM((lines, lanes), f32),
            pltpu.VMEM(project_weight.shape, bf16),
            pltpu.VMEM(residual.shape, bf16),
            pltpu.SemaphoreType.DMA((members + 1,)),
        ],
        1 << 29,
        project_weight, residual, own, from_last, from_far, from_next, norm_gain[None], pick,
        room=60, kept=2,
    )

    def exchanged(array):
        return lax.all_to_all(
            array.reshape(blocks, lines // blocks, lanes), "sp", split_axis=0, concat_axis=0,
            tiled=True,
        ).reshape(lines, lanes)

    landed = exchanged(outgoing)
    top, low = landed[: lines // 2], landed[lines // 2 :]
    last_top = moved(top, right)
    next_low = moved(low, left)
    last_low = moved(low, right)
    next_top = moved(top, left)
    far_top = moved(last_top, right)
    far_low = moved(next_low, left)

    def hidden_of(upper, lower):
        return call(
            hidden_kernel, shape((slots, gate_weight.shape[2]), bf16),
            [pltpu.VMEM((lines // 2, lanes), f32)], 1 << 29,
            upper, lower, gate_weight[0], linear_weight[0],
        )

    hidden_own = hidden_of(top, low)
    hidden_last = moved(hidden_of(last_top, last_low), left)
    hidden_next = moved(hidden_of(next_top, next_low), right)
    hidden_far = moved(hidden_of(far_top, far_low), across)
    summed = call(
        down_kernel, shape((slots, model), f32), [], 1 << 29,
        hidden_own, hidden_next, hidden_last, down, down_last, down_next,
    )
    answers = call(
        answer_kernel, shape((lines, lanes), bf16), [pltpu.VMEM((lines, lanes), f32)], 1 << 28,
        summed, hidden_far, down_far_top, down_far_low,
    )
    returned = exchanged(answers)
    return call(
        final_kernel, shape((share, model), bf16), [pltpu.VMEM((lines, lanes), f32)], 1 << 28,
        returned, mix, middle, final_gain[None],
    )


def solution(mesh):
    placed = (
        P(("sp", "tp"), None), P("sp", "tp"), P("sp", "tp"),
        P(None, "tp", None), P(None, "tp", None),
        P(None, "tp", None, None), P(None, "tp", None, None),
        P(None, "tp", None, None), P(None, "tp", None, None),
        P("tp"), P(), P(), P(),
        P("sp", None), P("sp"), P("sp", None),
        P("sp", None, "tp"), P("sp", None, "tp"), P("sp", "tp", None),
    )

    return jax.shard_map(
        on_device, mesh=mesh, in_specs=placed, out_specs=P(("sp", "tp"), None), check_vma=False
    )
```

```python
import jax
import jax.numpy as jnp
from jax import lax
from jax.experimental import pallas as pl
from jax.experimental.pallas import tpu as pltpu
from jax.sharding import PartitionSpec as P


deep_alpha = 2.0**0.25
norm_epsilon = 1e-05
f32 = jnp.float32
bf16 = jnp.bfloat16
VMEM = pltpu.MemorySpace.VMEM
lanes = 128
gate_row = 8
sent_rows = 9


def iota(shape, dim):
    return lax.broadcasted_iota(jnp.int32, shape, dim)


def mm(a, b):
    return lax.dot_general(a, b, (((1,), (0,)), ((), ())), preferred_element_type=f32)


def mm_nt(a, b):
    return lax.dot_general(a, b, (((1,), (1,)), ((), ())), preferred_element_type=f32)


def mm_tn(a, b):
    return lax.dot_general(a, b, (((0,), (0,)), ((), ())), preferred_element_type=f32)


def split(value, pieces):
    found = []
    for _ in range(pieces - 1):
        high = value.astype(bf16)
        found.append(high)
        value = value - high.astype(f32)
    return found + [value.astype(bf16)]


def exact_left(table, value):
    total = None
    for piece in split(value, 3):
        part = mm(table, piece)
        total = part if total is None else total + part
    return total


def exact_right(value, table):
    total = None
    for piece in split(value, 3):
        part = mm(piece, table)
        total = part if total is None else total + part
    return total


def reversal(size):
    return (iota((size, size), 0) + iota((size, size), 1) == size - 1).astype(f32).astype(bf16)


def as_row(table, groups, states):
    wide = jnp.concatenate([table] * groups, axis=1)
    keep = iota(wide.shape, 0) == iota(wide.shape, 1) // states
    return jnp.sum(jnp.where(keep, wide, 0.0), axis=0, keepdims=True)


def block_diagonal(table, groups, states):
    each = table.shape[0] // groups
    wide = jnp.concatenate([table] * groups, axis=1)
    keep = iota(wide.shape, 0) // each == iota(wide.shape, 1) // states
    return jnp.where(keep, wide, 0.0)


def steps_of(rate, turn, groups, states):
    retain = jnp.exp(-rate)
    return (
        as_row(retain * jnp.cos(turn), groups, states),
        as_row(retain * jnp.sin(turn), groups, states),
    )


def cmul(a, b):
    return (a[0] * b[0] - a[1] * b[1], a[0] * b[1] + a[1] * b[0])


def local_kernel(
    x_ref, gate_ref, rate_ref, turn_ref, drive_re_ref, drive_im_ref,
    send_ref, state_re_ref, state_im_ref, wide_ref, step_ref,
):
    length = x_ref.shape[0]
    groups, states = rate_ref.shape[1:]
    width = groups * states
    tiles = width // lanes
    turned = reversal(length)
    x = x_ref[...]
    log_gate = gate_ref[...]
    spread = (iota((groups, width), 0) == iota((groups, width), 1) // states).astype(f32).astype(bf16)
    factors = split(jnp.exp(log_gate), 3)
    for k in range(2):
        rate = rate_ref[k]
        step_re, step_im = steps_of(rate, turn_ref[k], groups, states)
        scale = as_row(jnp.sqrt(1.0 - jnp.exp(-2.0 * rate)), groups, states)
        x_k = x if k == 0 else mm(turned, x).astype(bf16)
        x_two = jnp.concatenate([x_k, x_k], axis=1)
        gates = None
        for piece in factors:
            piece_k = piece if k == 0 else mm(piece, turned).astype(bf16)
            part = mm_tn(piece_k, spread)
            gates = part if gates is None else gates + part
        pushes = []
        for drive_ref in (drive_re_ref, drive_im_ref):
            table = block_diagonal(drive_ref[k], groups, states) * scale
            pushes.append(mm(x_two, jnp.concatenate(split(table, 2), axis=0)))
        for j in range(tiles):
            cols = slice(j * lanes, (j + 1) * lanes)
            rows = pl.ds(k * tiles + j, length, stride=2 * tiles)
            wide_ref[rows, :] = gates[:, cols]
            state_re_ref[rows, :] = pushes[0][:, cols]
            state_im_ref[rows, :] = pushes[1][:, cols]
            at = k * tiles + j
            step_ref[at : at + 1, :] = step_re[:, cols]
            step_ref[2 * tiles + at : 2 * tiles + at + 1, :] = step_im[:, cols]
    high = 2 * tiles
    w_re = step_ref[0:high, :]
    w_im = step_ref[high : 2 * high, :]

    def advance(t, carried):
        re, im = carried
        at = pl.ds(pl.multiple_of(t * high, high), high)
        factor = wide_ref[at, :]
        a_re, a_im = factor * w_re, factor * w_im
        new_re = (state_re_ref[at, :] + a_re * re) - a_im * im
        new_im = (state_im_ref[at, :] + a_re * im) + a_im * re
        state_re_ref[at, :] = new_re
        state_im_ref[at, :] = new_im
        return new_re, new_im

    zero = jnp.zeros((high, lanes), f32)
    re, im = lax.fori_loop(0, length, advance, (zero, zero), unroll=8)
    step_ref[0:high, :] = re
    step_ref[high : 2 * high, :] = im
    blocks = send_ref.shape[0] // sent_rows
    later = iota((blocks, lanes), 0) > lax.axis_index("sp")
    for part in range(2):
        for j in range(tiles):
            forward = step_ref[part * high + j : part * high + j + 1, :]
            backward = step_ref[part * high + tiles + j : part * high + tiles + j + 1, :]
            send_ref[pl.ds(part * tiles + j, blocks, stride=sent_rows), :] = jnp.where(
                later, forward, backward
            )
    total = jnp.sum(log_gate, axis=1, keepdims=True)
    thin = iota((groups, lanes), 0) == iota((groups, lanes), 1) // (lanes // groups)
    total_row = jnp.sum(jnp.where(thin, total, 0.0), axis=0, keepdims=True)
    send_ref[pl.ds(gate_row, blocks, stride=sent_rows), :] = jnp.broadcast_to(
        total_row, (blocks, lanes)
    )


def powers(step, length, backward):
    width = step[0].shape[1]
    exponent = iota((8, width), 0)
    exponent = 8 - exponent if backward else exponent + 1
    current = step
    rows = (jnp.ones((8, width), f32), jnp.zeros((8, width), f32))
    for bit in range(4):
        taken = (exponent >> bit) % 2 == 1
        more = cmul(rows, current)
        rows = tuple(jnp.where(taken, m, r) for m, r in zip(more, rows))
        if bit < 3:
            current = cmul(current, current)
    grown = {8: (rows, current)}
    size = 8
    while size * 2 <= length:
        rows, current = grown[size]
        more = cmul(rows, current)
        pair = (more, rows) if backward else (rows, more)
        rows = tuple(jnp.concatenate([a, b], axis=0) for a, b in zip(*pair))
        grown[size * 2] = (rows, cmul(current, current))
        size *= 2
    rows, current = grown[size]
    rest = length - size
    if rest:
        tail_rows, tail_power = grown[rest]
        more = cmul(tail_rows, current)
        pair = (more, rows) if backward else (rows, more)
        rows = tuple(jnp.concatenate([a, b], axis=0) for a, b in zip(*pair))
        current = cmul(current, tail_power)
    return rows, current


def powers_at(step, exponents, most):
    rows = (jnp.ones(exponents.shape, f32), jnp.zeros(exponents.shape, f32))
    bit = 0
    while (1 << bit) <= most:
        taken = (exponents >> bit) % 2 == 1
        more = cmul(rows, step)
        rows = tuple(jnp.where(taken, m, r) for m, r in zip(more, rows))
        step = cmul(step, step)
        bit += 1
    return rows


def beside_kernel(
    x_ref, rate_ref, turn_ref, read_re_ref, read_im_ref, skip_ref,
    state_re_ref, state_im_ref, routes_ref, group_ref, weight_ref,
    local_ref, chain_ref, pick_ref, mix_ref,
):
    length = x_ref.shape[0]
    groups, states = rate_ref.shape[1:]
    width = groups * states
    tiles = width // lanes
    blocks = chain_ref.shape[1]
    here = lax.axis_index("sp")
    rows, cols = iota((length, length), 0), iota((length, length), 1)
    outs, wholes = [], []
    for k in range(2):
        total = None
        for part, state_ref in enumerate((state_re_ref, state_im_ref)):
            read_ref = (read_re_ref, read_im_ref)[part]
            table_high, table_low = split(block_diagonal(read_ref[k], groups, states), 2)
            for j in range(tiles):
                state = state_ref[pl.ds(k * tiles + j, length, stride=2 * tiles), :]
                state_high, state_low = split(state, 2)
                lane = slice(j * lanes, (j + 1) * lanes)
                value = (
                    mm_nt(state_high, table_high[:, lane])
                    + mm_nt(state_low, table_high[:, lane])
                    + mm_nt(state_high, table_low[:, lane])
                )
                if part:
                    value = -value
                total = value if total is None else total + value
        outs.append(total)
        step = steps_of(rate_ref[k], turn_ref[k], groups, states)
        whole = powers_at(step, jnp.full((1, width), length, jnp.int32), length)
        wholes.append(whole)
    source = iota((blocks, width), 0)
    earlier = source < here
    gap = jnp.where(earlier, here - 1 - source, source - 1 - here)
    whole = tuple(jnp.where(earlier, a, b) for a, b in zip(*wholes))
    chained = powers_at(whole, jnp.maximum(gap, 0), blocks - 1)
    for part in range(2):
        chain_ref[part] = jnp.where(gap >= 0, chained[part], 0.0)
    local_ref[...] = (
        outs[0] + exact_left(reversal(length), outs[1]) + skip_ref[...] * x_ref[...].astype(f32)
    )
    slots, share = pick_ref.shape
    routes = routes_ref[...]
    weights = weight_ref[...]
    scaled = group_ref[...] * weights / (weights[0:1] + weights[1:2])
    place = iota((slots, length), 0)
    first = routes[0:1] == place // 2
    second = routes[1:2] == place // 2
    named = jnp.where(first | second, 1.0, 0.0)
    before = (rows < cols) & (rows // share == cols // share)
    prior = mm(named.astype(bf16), before.astype(f32).astype(bf16))
    picked = jnp.where(prior == (place % 2).astype(f32), named, 0.0)
    base = lax.axis_index("tp") * share
    own = (iota((length, share), 0) == base + iota((length, share), 1)).astype(f32).astype(bf16)
    pick_ref[...] = mm(picked.astype(bf16), own).astype(bf16)
    own = (iota((share, length), 1) == base + iota((share, length), 0)).astype(f32).astype(bf16)
    mixing = None
    for piece in split(picked * jnp.where(first, scaled[0:1], scaled[1:2]), 3):
        more = mm_nt(own, piece)
        mixing = more if mixing is None else mixing + more
    mix_ref[...] = mixing


def carry_kernel(
    come_ref, local_ref, gate_ref, chain_ref, rate_ref, turn_ref, read_re_ref, read_im_ref,
    own_ref, next_ref, last_ref, far_ref, act_ref,
):
    here, member = lax.axis_index("sp"), lax.axis_index("tp")
    blocks, width = chain_ref.shape[1:]
    groups, states = rate_ref.shape[1:]
    tiles = width // lanes
    length = local_ref.shape[0]
    came = [
        jnp.concatenate(
            [come_ref[pl.ds(p * tiles + j, blocks, stride=sent_rows), :] for j in range(tiles)],
            axis=1,
        )
        for p in range(2)
    ]
    logs = come_ref[pl.ds(gate_row, blocks, stride=sent_rows), :]
    each = lanes // groups
    fan = (iota((lanes, width), 0) == each * (iota((lanes, width), 1) // states)).astype(f32)
    fan = fan.astype(bf16)
    thin = (iota((groups, lanes), 0) == iota((groups, lanes), 1) // each).astype(f32).astype(bf16)
    source, mid = iota((blocks, blocks), 0), iota((blocks, blocks), 1)
    rows, cols = iota((length, length), 0), iota((length, length), 1)
    between = ((mid > source) & (mid < here)) | ((mid < source) & (mid > here))
    between = jnp.where(between & (source != here), 1.0, 0.0).astype(bf16)
    fade = exact_right(jnp.exp(exact_left(between, logs)), fan)
    gathered = cmul((chain_ref[0] * fade, chain_ref[1] * fade), came)
    earlier = iota((blocks, width), 0) < here
    total = local_ref[...]
    for k in range(2):
        taken = earlier if k == 0 else ~earlier
        carry = [jnp.sum(jnp.where(taken, v, 0.0), axis=0, keepdims=True) for v in gathered]
        real = block_diagonal(read_re_ref[k], groups, states)
        imaginary = block_diagonal(read_im_ref[k], groups, states)
        step = steps_of(rate_ref[k], turn_ref[k], groups, states)
        grown, _ = powers(step, length, k == 1)
        first = carry[0] * real - carry[1] * imaginary
        second = -(carry[0] * imaginary + carry[1] * real)
        value = None
        for part, side in enumerate((first, second)):
            side_high, side_low = split(side, 2)
            high, low = split(grown[part], 2)
            more = mm_nt(high, side_high) + mm_nt(low, side_high) + mm_nt(high, side_low)
            value = more if value is None else value + more
        seen = (rows <= cols) if k == 0 else (rows >= cols)
        fade = jnp.exp(exact_right(gate_ref[...], seen.astype(f32).astype(bf16)))
        run = None
        for piece in split(fade, 3):
            more = mm_tn(piece, thin)
            run = more if run is None else run + more
        total = total + run * value
    act_ref[...] = jax.nn.gelu(total).astype(bf16)
    share = own_ref.shape[0]
    members = act_ref.shape[0] // share
    for shift, out_ref in enumerate((own_ref, next_ref, far_ref, last_ref)):
        at = lax.rem(member + shift, members) * share
        out_ref[...] = act_ref[pl.ds(pl.multiple_of(at, share), share), :]


def normed(values, gain):
    center = values - jnp.mean(values, axis=-1, keepdims=True)
    spread = jnp.mean(center * center, axis=-1, keepdims=True)
    return center * lax.rsqrt(spread + norm_epsilon) * gain


def to_lines(rows, rows_ref, out_ref):
    count, width = rows.shape
    each = width // lanes
    for q in range(each):
        rows_ref[pl.ds(q, count, stride=each), :] = rows[:, q * lanes : (q + 1) * lanes]
    out_ref[...] = rows_ref[...].astype(bf16)


def from_lines(lines_ref, rows_ref, each):
    count = lines_ref.shape[0] // each
    rows_ref[...] = lines_ref[...].astype(f32)
    return [rows_ref[pl.ds(q, count, stride=each), :].astype(bf16) for q in range(each)]


def branch_kernel(
    own_ref, from_last_ref, from_far_ref, from_next_ref, weight_ref, residual_ref, gain_ref,
    pick_ref, middle_ref, out_ref, rows_ref,
):
    member = lax.axis_index("tp")
    channels = own_ref.shape[1]
    members = weight_ref.shape[0] // channels
    branch = None
    for shift, part_ref in enumerate((own_ref, from_next_ref, from_far_ref, from_last_ref)):
        at = lax.rem(member + shift, members) * channels
        more = mm(part_ref[...], weight_ref[pl.ds(pl.multiple_of(at, channels), channels), :])
        branch = more if branch is None else branch + more
    middle = normed(deep_alpha * residual_ref[...].astype(f32) + branch, gain_ref[...])
    middle_ref[...] = middle
    to_lines(mm(pick_ref[...], middle.astype(bf16)), rows_ref, out_ref)


def hidden_kernel(top_ref, low_ref, gate_ref, linear_ref, out_ref, rows_ref):
    each = gate_ref.shape[0] // lanes
    half = top_ref.shape[0] // each
    for at, ref in ((0, top_ref), (half, low_ref)):
        rows = jnp.concatenate(from_lines(ref, rows_ref, each), axis=1)
        gate = mm(rows, gate_ref[...])
        linear = mm(rows, linear_ref[...])
        out_ref[at : at + half, :] = (jax.nn.silu(gate) * linear).astype(bf16)


def down_kernel(own_ref, last_ref, next_ref, w_own_ref, w_last_ref, w_next_ref, out_ref):
    total = mm(own_ref[...], w_own_ref[...]).astype(bf16).astype(f32)
    total = total + mm(last_ref[...], w_last_ref[...]).astype(bf16).astype(f32)
    out_ref[...] = total + mm(next_ref[...], w_next_ref[...]).astype(bf16).astype(f32)


def answer_kernel(sum_ref, far_ref, w_far_top_ref, w_far_low_ref, out_ref, rows_ref):
    half = w_far_top_ref.shape[0]
    far = mm(far_ref[:, :half], w_far_top_ref[...]) + mm(far_ref[:, half:], w_far_low_ref[...])
    to_lines(sum_ref[...] + far.astype(bf16).astype(f32), rows_ref, out_ref)


def final_kernel(answers_ref, mix_ref, middle_ref, gain_ref, out_ref, rows_ref):
    each = middle_ref.shape[1] // lanes
    mixing = split(mix_ref[...], 3)
    routed = []
    for answers in from_lines(answers_ref, rows_ref, each):
        routed.append(mm(mixing[0], answers) + mm(mixing[1], answers) + mm(mixing[2], answers))
    routed = jnp.concatenate(routed, axis=1)
    out_ref[...] = normed(deep_alpha * middle_ref[...] + routed, gain_ref[...]).astype(bf16)


def shape(dims, dtype):
    return jax.ShapeDtypeStruct(dims, dtype)


def call(kernel, outs, scratch, cost, *args, room=16, kept=0):
    many = isinstance(outs, (list, tuple))
    whole = pl.BlockSpec(memory_space=VMEM)
    return pl.pallas_call(
        kernel,
        out_shape=outs,
        in_specs=[pl.BlockSpec(memory_space=pl.ANY)] * kept + [whole] * (len(args) - kept),
        out_specs=[whole] * len(outs) if many else whole,
        scratch_shapes=scratch,
        compiler_params=pltpu.CompilerParams(vmem_limit_bytes=room << 20),
        cost_estimate=pl.CostEstimate(flops=cost, bytes_accessed=1 << 20, transcendentals=0),
    )(*args)


def on_device(
    residual, mixer_input, log_gate, decay_rate, turn_rate, drive_real, drive_imaginary,
    read_real, read_imaginary, skip_gain, project_weight, norm_gain, final_gain, routes,
    group_weight, expert_weight, gate_weight, linear_weight, down_weight,
):
    length, channels = mixer_input.shape
    groups, states = decay_rate.shape[1:]
    width = groups * states
    share, model = residual.shape
    blocks = lax.axis_size("sp")
    members = lax.axis_size("tp")
    slots = 2 * blocks
    right = [(i, (i + 1) % members) for i in range(members)]
    left = [(i, (i - 1) % members) for i in range(members)]
    across = [(i, (i + 2) % members) for i in range(members)]

    def moved(array, way):
        return lax.ppermute(array, "tp", way)

    down = down_weight[0]
    half_down = down.shape[0] // 2
    down_last = moved(down, right)
    down_next = moved(down, left)

    flat = lambda table: table.reshape(2, -1, states)
    send, state_re, state_im = call(
        local_kernel,
        [
            shape((blocks * sent_rows, lanes), f32),
            shape((length * 2 * width // lanes, lanes), f32),
            shape((length * 2 * width // lanes, lanes), f32),
        ],
        [
            pltpu.VMEM((length * 2 * width // lanes, lanes), f32),
            pltpu.VMEM((4 * width // lanes, lanes), f32),
        ],
        1 << 30,
        mixer_input, log_gate.T, decay_rate, turn_rate, flat(drive_real), flat(drive_imaginary),
        room=60,
    )
    come = lax.all_to_all(
        send.reshape(blocks, 1, sent_rows * lanes), "sp", split_axis=0, concat_axis=0,
        tiled=True,
    ).reshape(blocks * sent_rows, lanes)
    local, chain, pick, mix = call(
        beside_kernel,
        [
            shape((length, lanes), f32),
            shape((2, blocks, width), f32),
            shape((slots, share), bf16),
            shape((share, slots), f32),
        ],
        [],
        1 << 30,
        mixer_input, decay_rate, turn_rate, flat(read_real), flat(read_imaginary),
        skip_gain[None], state_re, state_im, routes.T, group_weight[None], expert_weight.T,
        room=40,
    )
    own, to_next, to_last, to_far = call(
        carry_kernel,
        [shape((share, channels), bf16)] * 4,
        [pltpu.VMEM((length, channels), bf16)],
        1 << 29,
        come, local, log_gate.T, chain, decay_rate, turn_rate, flat(read_real), flat(read_imaginary),
        room=40,
    )
    from_far = moved(to_far, across)
    from_last = moved(to_next, right)
    from_next = moved(to_last, left)
    down_far_top = moved(down_last[:half_down], right)
    down_far_low = moved(down_next[half_down:], left)
    lines = slots * model // lanes
    middle, outgoing = call(
        branch_kernel,
        [shape((share, model), f32), shape((lines, lanes), bf16)],
        [pltpu.VMEM((lines, lanes), f32)],
        1 << 29,
        own, from_last, from_far, from_next, project_weight, residual, norm_gain[None], pick,
    )

    def exchanged(array):
        return lax.all_to_all(
            array.reshape(blocks, lines // blocks, lanes), "sp", split_axis=0, concat_axis=0,
            tiled=True,
        ).reshape(lines, lanes)

    landed = exchanged(outgoing)
    top, low = landed[: lines // 2], landed[lines // 2 :]
    last_top = moved(top, right)
    next_low = moved(low, left)
    last_low = moved(low, right)
    next_top = moved(top, left)
    far_top = moved(last_top, right)
    far_low = moved(next_low, left)

    def hidden_of(upper, lower):
        return call(
            hidden_kernel, shape((slots, gate_weight.shape[2]), bf16),
            [pltpu.VMEM((lines // 2, lanes), f32)], 1 << 29,
            upper, lower, gate_weight[0], linear_weight[0],
        )

    hidden_own = hidden_of(top, low)
    hidden_last = moved(hidden_of(last_top, last_low), left)
    hidden_next = moved(hidden_of(next_top, next_low), right)
    hidden_far = moved(hidden_of(far_top, far_low), across)
    summed = call(
        down_kernel, shape((slots, model), f32), [], 1 << 29,
        hidden_own, hidden_next, hidden_last, down, down_last, down_next,
    )
    answers = call(
        answer_kernel, shape((lines, lanes), bf16), [pltpu.VMEM((lines, lanes), f32)], 1 << 28,
        summed, hidden_far, down_far_top, down_far_low,
    )
    returned = exchanged(answers)
    return call(
        final_kernel, shape((share, model), bf16), [pltpu.VMEM((lines, lanes), f32)], 1 << 28,
        returned, mix, middle, final_gain[None],
    )


def solution(mesh):
    placed = (
        P(("sp", "tp"), None), P("sp", "tp"), P("sp", "tp"),
        P(None, "tp", None), P(None, "tp", None),
        P(None, "tp", None, None), P(None, "tp", None, None),
        P(None, "tp", None, None), P(None, "tp", None, None),
        P("tp"), P(), P(), P(),
        P("sp", None), P("sp"), P("sp", None),
        P("sp", None, "tp"), P("sp", None, "tp"), P("sp", "tp", None),
    )

    return jax.shard_map(
        on_device, mesh=mesh, in_specs=placed, out_specs=P(("sp", "tp"), None), check_vma=False
    )
```

```python
import jax
import jax.numpy as jnp
from jax import lax
from jax.experimental import pallas as pl
from jax.experimental.pallas import tpu as pltpu
from jax.sharding import PartitionSpec as P


deep_alpha = 2.0**0.25
norm_epsilon = 1e-05
f32 = jnp.float32
bf16 = jnp.bfloat16
VMEM = pltpu.MemorySpace.VMEM
lanes = 128


def iota(shape, dim):
    return lax.broadcasted_iota(jnp.int32, shape, dim)


def mm(a, b):
    return lax.dot_general(a, b, (((1,), (0,)), ((), ())), preferred_element_type=f32)


def mm_nt(a, b):
    return lax.dot_general(a, b, (((1,), (1,)), ((), ())), preferred_element_type=f32)


def mm_tn(a, b):
    return lax.dot_general(a, b, (((0,), (0,)), ((), ())), preferred_element_type=f32)


def split(value, pieces):
    found = []
    for _ in range(pieces - 1):
        high = value.astype(bf16)
        found.append(high)
        value = value - high.astype(f32)
    return found + [value.astype(bf16)]


def exact_left(table, value):
    total = None
    for piece in split(value, 3):
        part = mm(table, piece)
        total = part if total is None else total + part
    return total


def exact_right(value, table):
    total = None
    for piece in split(value, 3):
        part = mm(piece, table)
        total = part if total is None else total + part
    return total


def reversal(size):
    return (iota((size, size), 0) + iota((size, size), 1) == size - 1).astype(f32).astype(bf16)


def as_row(table, groups, states):
    wide = jnp.concatenate([table] * groups, axis=1)
    keep = iota(wide.shape, 0) == iota(wide.shape, 1) // states
    return jnp.sum(jnp.where(keep, wide, 0.0), axis=0, keepdims=True)


def block_diagonal(table, groups, states):
    each = table.shape[0] // groups
    wide = jnp.concatenate([table] * groups, axis=1)
    keep = iota(wide.shape, 0) // each == iota(wide.shape, 1) // states
    return jnp.where(keep, wide, 0.0)


def steps_of(rate, turn, groups, states):
    retain = jnp.exp(-rate)
    return (
        as_row(retain * jnp.cos(turn), groups, states),
        as_row(retain * jnp.sin(turn), groups, states),
    )


def cmul(a, b):
    return (a[0] * b[0] - a[1] * b[1], a[0] * b[1] + a[1] * b[0])


def pushed(
    x_ref, gate_ref, rate_ref, turn_ref, drive_re_ref, drive_im_ref,
    push_re_ref, push_im_ref, wide_ref, step_ref,
):
    length = x_ref.shape[0]
    groups, states = rate_ref.shape[1:]
    width = groups * states
    tiles = width // lanes
    turned = reversal(length)
    x = x_ref[...]
    spread = (iota((groups, width), 0) == iota((groups, width), 1) // states).astype(f32).astype(bf16)
    factors = split(jnp.exp(gate_ref[...]), 3)
    for k in range(2):
        rate = rate_ref[k]
        step_re, step_im = steps_of(rate, turn_ref[k], groups, states)
        scale = as_row(jnp.sqrt(1.0 - jnp.exp(-2.0 * rate)), groups, states)
        x_k = x if k == 0 else mm(turned, x).astype(bf16)
        x_two = jnp.concatenate([x_k, x_k], axis=1)
        gates = None
        for piece in factors:
            piece_k = piece if k == 0 else mm(piece, turned).astype(bf16)
            part = mm_tn(piece_k, spread)
            gates = part if gates is None else gates + part
        pushes = []
        for drive_ref in (drive_re_ref, drive_im_ref):
            table = block_diagonal(drive_ref[k], groups, states) * scale
            pushes.append(mm(x_two, jnp.concatenate(split(table, 2), axis=0)))
        for j in range(tiles):
            cols = slice(j * lanes, (j + 1) * lanes)
            rows = pl.ds(k * tiles + j, length, stride=2 * tiles)
            wide_ref[rows, :] = gates[:, cols]
            push_re_ref[rows, :] = pushes[0][:, cols]
            push_im_ref[rows, :] = pushes[1][:, cols]
            at = k * tiles + j
            step_ref[at : at + 1, :] = step_re[:, cols]
            step_ref[2 * tiles + at : 2 * tiles + at + 1, :] = step_im[:, cols]


def local_kernel(
    x_ref, gate_ref, rate_ref, turn_ref, drive_re_ref, drive_im_ref,
    send_ref, push_re_ref, push_im_ref, wide_ref, step_ref, pair_ref,
):
    pushed(
        x_ref, gate_ref, rate_ref, turn_ref, drive_re_ref, drive_im_ref,
        push_re_ref, push_im_ref, wide_ref, step_ref,
    )
    groups = rate_ref.shape[1]
    high = step_ref.shape[0] // 2
    tiles = high // 2
    half = x_ref.shape[0] // 2
    w = (step_ref[0:high, :], step_ref[high : 2 * high, :])

    def advance(t, carried):
        states = []
        for side, (re, im) in enumerate(carried[:2]):
            at = pl.ds(pl.multiple_of((t + side * half) * high, high), high)
            factor = wide_ref[at, :]
            a_re, a_im = factor * w[0], factor * w[1]
            states.append(
                (
                    (push_re_ref[at, :] + a_re * re) - a_im * im,
                    (push_im_ref[at, :] + a_re * im) + a_im * re,
                )
            )
        return (*states, cmul((a_re, a_im), carried[2]))

    zero, one = jnp.zeros((high, lanes), f32), jnp.ones((high, lanes), f32)
    early, late, faded = lax.fori_loop(
        0, half, advance, ((zero, zero), (zero, zero), (one, zero)), unroll=8
    )
    whole = cmul(faded, early)
    step_ref[0:high, :] = late[0] + whole[0]
    step_ref[high : 2 * high, :] = late[1] + whole[1]
    total = jnp.sum(gate_ref[...], axis=1, keepdims=True)
    thin = iota((groups, lanes), 0) == iota((groups, lanes), 1) // (lanes // groups)
    total = jnp.sum(jnp.where(thin, total, 0.0), axis=0, keepdims=True)
    total_high = total.astype(bf16).astype(f32)
    for k in range(2):
        for part, rest in enumerate((total_high, total - total_high)):
            at = 2 * k + part
            for j in range(tiles):
                row = part * high + k * tiles + j
                pair_ref[at : at + 1, j * lanes : (j + 1) * lanes] = step_ref[row : row + 1, :]
            pair_ref[at : at + 1, tiles * lanes :] = rest
    forward, backward = pair_ref[0:2, :], pair_ref[2:4, :]
    here = lax.axis_index("sp")
    for block in range(send_ref.shape[0]):
        send_ref[block] = jnp.where(block > here, forward, backward).astype(bf16)


def powers(step, length, backward):
    width = step[0].shape[1]
    exponent = iota((8, width), 0)
    exponent = 8 - exponent if backward else exponent + 1
    current = step
    rows = (jnp.ones((8, width), f32), jnp.zeros((8, width), f32))
    for bit in range(4):
        taken = (exponent >> bit) % 2 == 1
        more = cmul(rows, current)
        rows = tuple(jnp.where(taken, m, r) for m, r in zip(more, rows))
        if bit < 3:
            current = cmul(current, current)
    grown = {8: (rows, current)}
    size = 8
    while size * 2 <= length:
        rows, current = grown[size]
        more = cmul(rows, current)
        pair = (more, rows) if backward else (rows, more)
        rows = tuple(jnp.concatenate([a, b], axis=0) for a, b in zip(*pair))
        grown[size * 2] = (rows, cmul(current, current))
        size *= 2
    rows, current = grown[size]
    rest = length - size
    if rest:
        tail_rows, tail_power = grown[rest]
        more = cmul(tail_rows, current)
        pair = (more, rows) if backward else (rows, more)
        rows = tuple(jnp.concatenate([a, b], axis=0) for a, b in zip(*pair))
        current = cmul(current, tail_power)
    return rows, current


def powers_at(step, exponents, most):
    rows = (jnp.ones(exponents.shape, f32), jnp.zeros(exponents.shape, f32))
    bit = 0
    while (1 << bit) <= most:
        taken = (exponents >> bit) % 2 == 1
        more = cmul(rows, step)
        rows = tuple(jnp.where(taken, m, r) for m, r in zip(more, rows))
        step = cmul(step, step)
        bit += 1
    return rows


def beside_kernel(
    x_ref, gate_ref, rate_ref, turn_ref, drive_re_ref, drive_im_ref, read_re_ref, read_im_ref,
    skip_ref, routes_ref, group_ref, weight_ref,
    local_ref, chain_ref, pick_ref, mix_ref,
    state_re_ref, state_im_ref, wide_ref, step_ref,
):
    length = x_ref.shape[0]
    groups, states = rate_ref.shape[1:]
    width = groups * states
    tiles = width // lanes
    blocks = chain_ref.shape[1]
    here = lax.axis_index("sp")
    pushed(
        x_ref, gate_ref, rate_ref, turn_ref, drive_re_ref, drive_im_ref,
        state_re_ref, state_im_ref, wide_ref, step_ref,
    )
    high = 2 * tiles
    w_re = step_ref[0:high, :]
    w_im = step_ref[high : 2 * high, :]

    def advance(t, carried):
        re, im = carried
        at = pl.ds(pl.multiple_of(t * high, high), high)
        factor = wide_ref[at, :]
        a_re, a_im = factor * w_re, factor * w_im
        new_re = (state_re_ref[at, :] + a_re * re) - a_im * im
        new_im = (state_im_ref[at, :] + a_re * im) + a_im * re
        state_re_ref[at, :] = new_re
        state_im_ref[at, :] = new_im
        return new_re, new_im

    zero = jnp.zeros((high, lanes), f32)
    lax.fori_loop(0, length, advance, (zero, zero), unroll=8)
    rows, cols = iota((length, length), 0), iota((length, length), 1)
    outs, wholes = [], []
    for k in range(2):
        total = None
        for part, state_ref in enumerate((state_re_ref, state_im_ref)):
            read_ref = (read_re_ref, read_im_ref)[part]
            table_high, table_low = split(block_diagonal(read_ref[k], groups, states), 2)
            for j in range(tiles):
                state = state_ref[pl.ds(k * tiles + j, length, stride=2 * tiles), :]
                state_high, state_low = split(state, 2)
                lane = slice(j * lanes, (j + 1) * lanes)
                value = (
                    mm_nt(state_high, table_high[:, lane])
                    + mm_nt(state_low, table_high[:, lane])
                    + mm_nt(state_high, table_low[:, lane])
                )
                if part:
                    value = -value
                total = value if total is None else total + value
        outs.append(total)
        step = steps_of(rate_ref[k], turn_ref[k], groups, states)
        whole = powers_at(step, jnp.full((1, width), length, jnp.int32), length)
        wholes.append(whole)
    source = iota((blocks, width), 0)
    earlier = source < here
    gap = jnp.where(earlier, here - 1 - source, source - 1 - here)
    whole = tuple(jnp.where(earlier, a, b) for a, b in zip(*wholes))
    chained = powers_at(whole, jnp.maximum(gap, 0), blocks - 1)
    for part in range(2):
        chain_ref[part] = jnp.where(gap >= 0, chained[part], 0.0)
    local_ref[...] = (
        outs[0] + exact_left(reversal(length), outs[1]) + skip_ref[...] * x_ref[...].astype(f32)
    )
    slots, share = pick_ref.shape
    routes = routes_ref[...]
    weights = weight_ref[...]
    scaled = group_ref[...] * weights / (weights[0:1] + weights[1:2])
    place = iota((slots, length), 0)
    first = routes[0:1] == place // 2
    second = routes[1:2] == place // 2
    named = jnp.where(first | second, 1.0, 0.0)
    before = (rows < cols) & (rows // share == cols // share)
    prior = mm(named.astype(bf16), before.astype(f32).astype(bf16))
    picked = jnp.where(prior == (place % 2).astype(f32), named, 0.0)
    base = lax.axis_index("tp") * share
    own = (iota((length, share), 0) == base + iota((length, share), 1)).astype(f32).astype(bf16)
    pick_ref[...] = mm(picked.astype(bf16), own).astype(bf16)
    own = (iota((share, length), 1) == base + iota((share, length), 0)).astype(f32).astype(bf16)
    mixing = None
    for piece in split(picked * jnp.where(first, scaled[0:1], scaled[1:2]), 3):
        more = mm_nt(own, piece)
        mixing = more if mixing is None else mixing + more
    mix_ref[...] = mixing


def carry_kernel(
    come_ref, local_ref, gate_ref, chain_ref, rate_ref, turn_ref, read_re_ref, read_im_ref,
    own_ref, next_ref, last_ref, far_ref, act_ref, lines_ref,
):
    here, member = lax.axis_index("sp"), lax.axis_index("tp")
    blocks, width = chain_ref.shape[1:]
    groups, states = rate_ref.shape[1:]
    tiles = width // lanes
    length = local_ref.shape[0]
    for block in range(blocks):
        pair = come_ref[block].astype(f32)
        for j in range(tiles + 1):
            at = 2 * (j * blocks + block)
            lines_ref[at : at + 2, :] = pair[:, j * lanes : (j + 1) * lanes]

    def lines_of(part, j):
        return lines_ref[pl.ds(2 * j * blocks + part, blocks, stride=2), :]

    came = [
        jnp.concatenate([lines_of(part, j) for j in range(tiles)], axis=1) for part in range(2)
    ]
    logs = lines_of(0, tiles) + lines_of(1, tiles)
    each = lanes // groups
    fan = (iota((lanes, width), 0) == each * (iota((lanes, width), 1) // states)).astype(f32)
    fan = fan.astype(bf16)
    thin = (iota((groups, lanes), 0) == iota((groups, lanes), 1) // each).astype(f32).astype(bf16)
    source, mid = iota((blocks, blocks), 0), iota((blocks, blocks), 1)
    rows, cols = iota((length, length), 0), iota((length, length), 1)
    between = ((mid > source) & (mid < here)) | ((mid < source) & (mid > here))
    between = jnp.where(between & (source != here), 1.0, 0.0).astype(bf16)
    fade = exact_right(jnp.exp(exact_left(between, logs)), fan)
    gathered = cmul((chain_ref[0] * fade, chain_ref[1] * fade), came)
    earlier = iota((blocks, width), 0) < here
    total = local_ref[...]
    for k in range(2):
        taken = earlier if k == 0 else ~earlier
        carry = [jnp.sum(jnp.where(taken, v, 0.0), axis=0, keepdims=True) for v in gathered]
        real = block_diagonal(read_re_ref[k], groups, states)
        imaginary = block_diagonal(read_im_ref[k], groups, states)
        step = steps_of(rate_ref[k], turn_ref[k], groups, states)
        grown, _ = powers(step, length, k == 1)
        first = carry[0] * real - carry[1] * imaginary
        second = -(carry[0] * imaginary + carry[1] * real)
        value = None
        for part, side in enumerate((first, second)):
            side_high, side_low = split(side, 2)
            high, low = split(grown[part], 2)
            more = mm_nt(high, side_high) + mm_nt(low, side_high) + mm_nt(high, side_low)
            value = more if value is None else value + more
        seen = (rows <= cols) if k == 0 else (rows >= cols)
        fade = jnp.exp(exact_right(gate_ref[...], seen.astype(f32).astype(bf16)))
        run = None
        for piece in split(fade, 3):
            more = mm_tn(piece, thin)
            run = more if run is None else run + more
        total = total + run * value
    act_ref[...] = jax.nn.gelu(total).astype(bf16)
    share = own_ref.shape[0]
    members = act_ref.shape[0] // share
    for shift, out_ref in enumerate((own_ref, next_ref, far_ref, last_ref)):
        at = lax.rem(member + shift, members) * share
        out_ref[...] = act_ref[pl.ds(pl.multiple_of(at, share), share), :]


def normed(values, gain):
    center = values - jnp.mean(values, axis=-1, keepdims=True)
    spread = jnp.mean(center * center, axis=-1, keepdims=True)
    return center * lax.rsqrt(spread + norm_epsilon) * gain


def to_lines(rows, rows_ref, out_ref):
    count, width = rows.shape
    each = width // lanes
    for q in range(each):
        rows_ref[pl.ds(q, count, stride=each), :] = rows[:, q * lanes : (q + 1) * lanes]
    out_ref[...] = rows_ref[...].astype(bf16)


def from_lines(lines_ref, rows_ref, each):
    count = lines_ref.shape[0] // each
    rows_ref[...] = lines_ref[...].astype(f32)
    return [rows_ref[pl.ds(q, count, stride=each), :].astype(bf16) for q in range(each)]


def branch_kernel(
    own_ref, from_last_ref, from_far_ref, from_next_ref, weight_ref, residual_ref, gain_ref,
    pick_ref, middle_ref, out_ref, rows_ref,
):
    member = lax.axis_index("tp")
    channels = own_ref.shape[1]
    members = weight_ref.shape[0] // channels
    branch = None
    for shift, part_ref in enumerate((own_ref, from_next_ref, from_far_ref, from_last_ref)):
        at = lax.rem(member + shift, members) * channels
        more = mm(part_ref[...], weight_ref[pl.ds(pl.multiple_of(at, channels), channels), :])
        branch = more if branch is None else branch + more
    middle = normed(deep_alpha * residual_ref[...].astype(f32) + branch, gain_ref[...])
    middle_ref[...] = middle
    to_lines(mm(pick_ref[...], middle.astype(bf16)), rows_ref, out_ref)


def hidden_kernel(top_ref, low_ref, gate_ref, linear_ref, out_ref, rows_ref):
    each = gate_ref.shape[0] // lanes
    half = top_ref.shape[0] // each
    for at, ref in ((0, top_ref), (half, low_ref)):
        rows = jnp.concatenate(from_lines(ref, rows_ref, each), axis=1)
        gate = mm(rows, gate_ref[...])
        linear = mm(rows, linear_ref[...])
        out_ref[at : at + half, :] = (jax.nn.silu(gate) * linear).astype(bf16)


def down_kernel(own_ref, last_ref, next_ref, w_own_ref, w_last_ref, w_next_ref, out_ref):
    total = mm(own_ref[...], w_own_ref[...]).astype(bf16).astype(f32)
    total = total + mm(last_ref[...], w_last_ref[...]).astype(bf16).astype(f32)
    out_ref[...] = total + mm(next_ref[...], w_next_ref[...]).astype(bf16).astype(f32)


def answer_kernel(sum_ref, far_ref, w_far_ref, out_ref, rows_ref):
    far = mm(far_ref[...], w_far_ref[...])
    to_lines(sum_ref[...] + far.astype(bf16).astype(f32), rows_ref, out_ref)


def final_kernel(answers_ref, mix_ref, middle_ref, gain_ref, out_ref, rows_ref):
    each = middle_ref.shape[1] // lanes
    mixing = split(mix_ref[...], 3)
    routed = []
    for answers in from_lines(answers_ref, rows_ref, each):
        routed.append(mm(mixing[0], answers) + mm(mixing[1], answers) + mm(mixing[2], answers))
    routed = jnp.concatenate(routed, axis=1)
    out_ref[...] = normed(deep_alpha * middle_ref[...] + routed, gain_ref[...]).astype(bf16)


def shape(dims, dtype):
    return jax.ShapeDtypeStruct(dims, dtype)


def call(kernel, outs, scratch, cost, *args, room=16, kept=0):
    many = isinstance(outs, (list, tuple))
    whole = pl.BlockSpec(memory_space=VMEM)
    return pl.pallas_call(
        kernel,
        out_shape=outs,
        in_specs=[pl.BlockSpec(memory_space=pl.ANY)] * kept + [whole] * (len(args) - kept),
        out_specs=[whole] * len(outs) if many else whole,
        scratch_shapes=scratch,
        compiler_params=pltpu.CompilerParams(vmem_limit_bytes=room << 20),
        cost_estimate=pl.CostEstimate(flops=cost, bytes_accessed=1 << 20, transcendentals=0),
    )(*args)


def on_device(
    residual, mixer_input, log_gate, decay_rate, turn_rate, drive_real, drive_imaginary,
    read_real, read_imaginary, skip_gain, project_weight, norm_gain, final_gain, routes,
    group_weight, expert_weight, gate_weight, linear_weight, down_weight,
):
    length, channels = mixer_input.shape
    groups, states = decay_rate.shape[1:]
    width = groups * states
    share, model = residual.shape
    blocks = lax.axis_size("sp")
    members = lax.axis_size("tp")
    slots = 2 * blocks
    right = [(i, (i + 1) % members) for i in range(members)]
    left = [(i, (i - 1) % members) for i in range(members)]
    across = [(i, (i + 2) % members) for i in range(members)]

    def moved(array, way):
        return lax.ppermute(array, "tp", way)

    down = down_weight[0]
    down_last = moved(down, right)
    down_next = moved(down, left)

    flat = lambda table: table.reshape(2, -1, states)
    rows = length * 2 * width // lanes
    swept = [pltpu.VMEM((rows, lanes), f32)] * 3 + [pltpu.VMEM((4 * width // lanes, lanes), f32)]
    send = call(
        local_kernel, shape((blocks, 2, width + lanes), bf16),
        swept + [pltpu.VMEM((8, width + lanes), f32)], 1 << 30,
        mixer_input, log_gate.T, decay_rate, turn_rate, flat(drive_real),
        flat(drive_imaginary),
        room=60,
    )
    come = lax.all_to_all(send, "sp", split_axis=0, concat_axis=0, tiled=True)
    local, chain, pick, mix = call(
        beside_kernel,
        [
            shape((length, lanes), f32),
            shape((2, blocks, width), f32),
            shape((slots, share), bf16),
            shape((share, slots), f32),
        ],
        swept,
        1 << 30,
        mixer_input, log_gate.T, decay_rate, turn_rate, flat(drive_real),
        flat(drive_imaginary), flat(read_real), flat(read_imaginary), skip_gain[None], routes.T, group_weight[None], expert_weight.T,
        room=40,
    )
    own, to_next, to_last, to_far = call(
        carry_kernel,
        [shape((share, channels), bf16)] * 4,
        [
            pltpu.VMEM((length, channels), bf16),
            pltpu.VMEM((2 * blocks * (width // lanes + 1), lanes), f32),
        ],
        1 << 29,
        come, local, log_gate.T, chain, decay_rate, turn_rate, flat(read_real), flat(read_imaginary),
        room=40,
    )
    from_far = moved(to_far, across)
    from_last = moved(to_next, right)
    from_next = moved(to_last, left)
    down_far = moved(down_last, right)
    lines = slots * model // lanes
    middle, outgoing = call(
        branch_kernel,
        [shape((share, model), f32), shape((lines, lanes), bf16)],
        [pltpu.VMEM((lines, lanes), f32)],
        1 << 29,
        own, from_last, from_far, from_next, project_weight, residual, norm_gain[None], pick,
    )

    def exchanged(array):
        return lax.all_to_all(
            array.reshape(blocks, lines // blocks, lanes), "sp", split_axis=0, concat_axis=0,
            tiled=True,
        ).reshape(lines, lanes)

    landed = exchanged(outgoing)
    top, low = landed[: lines // 2], landed[lines // 2 :]
    last_top = moved(top, right)
    next_low = moved(low, left)
    last_low = moved(low, right)
    next_top = moved(top, left)
    far_top = moved(last_top, right)
    far_low = moved(next_low, left)

    def hidden_of(upper, lower):
        return call(
            hidden_kernel, shape((slots, gate_weight.shape[2]), bf16),
            [pltpu.VMEM((lines // 2, lanes), f32)], 1 << 29,
            upper, lower, gate_weight[0], linear_weight[0],
        )

    hidden_own = hidden_of(top, low)
    hidden_last = moved(hidden_of(last_top, last_low), left)
    hidden_next = moved(hidden_of(next_top, next_low), right)
    hidden_far = moved(hidden_of(far_top, far_low), across)
    summed = call(
        down_kernel, shape((slots, model), f32), [], 1 << 29,
        hidden_own, hidden_next, hidden_last, down, down_last, down_next,
    )
    answers = call(
        answer_kernel, shape((lines, lanes), bf16), [pltpu.VMEM((lines, lanes), f32)], 1 << 28,
        summed, hidden_far, down_far,
    )
    returned = exchanged(answers)
    return call(
        final_kernel, shape((share, model), bf16), [pltpu.VMEM((lines, lanes), f32)], 1 << 28,
        returned, mix, middle, final_gain[None],
    )


def solution(mesh):
    placed = (
        P(("sp", "tp"), None), P("sp", "tp"), P("sp", "tp"),
        P(None, "tp", None), P(None, "tp", None),
        P(None, "tp", None, None), P(None, "tp", None, None),
        P(None, "tp", None, None), P(None, "tp", None, None),
        P("tp"), P(), P(), P(),
        P("sp", None), P("sp"), P("sp", None),
        P("sp", None, "tp"), P("sp", None, "tp"), P("sp", "tp", None),
    )

    return jax.shard_map(
        on_device, mesh=mesh, in_specs=placed, out_specs=P(("sp", "tp"), None), check_vma=False
    )
```

```python
import jax
import jax.numpy as jnp
from jax import lax
from jax.experimental import pallas as pl
from jax.experimental.pallas import tpu as pltpu
from jax.sharding import PartitionSpec as P


deep_alpha = 2.0**0.25
norm_epsilon = 1e-05
f32 = jnp.float32
bf16 = jnp.bfloat16
VMEM = pltpu.MemorySpace.VMEM
lanes = 128


def iota(shape, dim):
    return lax.broadcasted_iota(jnp.int32, shape, dim)


def mm(a, b):
    return lax.dot_general(a, b, (((1,), (0,)), ((), ())), preferred_element_type=f32)


def mm_nt(a, b):
    return lax.dot_general(a, b, (((1,), (1,)), ((), ())), preferred_element_type=f32)


def mm_tn(a, b):
    return lax.dot_general(a, b, (((0,), (0,)), ((), ())), preferred_element_type=f32)


def split(value, pieces):
    found = []
    for _ in range(pieces - 1):
        high = value.astype(bf16)
        found.append(high)
        value = value - high.astype(f32)
    return found + [value.astype(bf16)]


def exact_left(table, value):
    total = None
    for piece in split(value, 3):
        part = mm(table, piece)
        total = part if total is None else total + part
    return total


def exact_right(value, table):
    total = None
    for piece in split(value, 3):
        part = mm(piece, table)
        total = part if total is None else total + part
    return total


def reversal(size):
    return (iota((size, size), 0) + iota((size, size), 1) == size - 1).astype(f32).astype(bf16)


def as_row(table, groups, states):
    wide = jnp.concatenate([table] * groups, axis=1)
    keep = iota(wide.shape, 0) == iota(wide.shape, 1) // states
    return jnp.sum(jnp.where(keep, wide, 0.0), axis=0, keepdims=True)


def block_diagonal(table, groups, states):
    each = table.shape[0] // groups
    wide = jnp.concatenate([table] * groups, axis=1)
    keep = iota(wide.shape, 0) // each == iota(wide.shape, 1) // states
    return jnp.where(keep, wide, 0.0)


def steps_of(rate, turn, groups, states):
    retain = jnp.exp(-rate)
    return (
        as_row(retain * jnp.cos(turn), groups, states),
        as_row(retain * jnp.sin(turn), groups, states),
    )


def cmul(a, b):
    return (a[0] * b[0] - a[1] * b[1], a[0] * b[1] + a[1] * b[0])


def pushed(
    x_ref, gate_ref, rate_ref, turn_ref, drive_re_ref, drive_im_ref,
    push_re_ref, push_im_ref, wide_ref, step_ref,
):
    length = x_ref.shape[0]
    groups, states = rate_ref.shape[1:]
    width = groups * states
    tiles = width // lanes
    turned = reversal(length)
    x = x_ref[...]
    spread = (iota((groups, width), 0) == iota((groups, width), 1) // states).astype(f32).astype(bf16)
    factors = split(jnp.exp(gate_ref[...]), 3)
    for k in range(2):
        rate = rate_ref[k]
        step_re, step_im = steps_of(rate, turn_ref[k], groups, states)
        scale = as_row(jnp.sqrt(1.0 - jnp.exp(-2.0 * rate)), groups, states)
        x_k = x if k == 0 else mm(turned, x).astype(bf16)
        x_two = jnp.concatenate([x_k, x_k], axis=1)
        gates = None
        for piece in factors:
            piece_k = piece if k == 0 else mm(piece, turned).astype(bf16)
            part = mm_tn(piece_k, spread)
            gates = part if gates is None else gates + part
        pushes = []
        for drive_ref in (drive_re_ref, drive_im_ref):
            table = block_diagonal(drive_ref[k], groups, states) * scale
            pushes.append(mm(x_two, jnp.concatenate(split(table, 2), axis=0)))
        for j in range(tiles):
            cols = slice(j * lanes, (j + 1) * lanes)
            rows = pl.ds(k * tiles + j, length, stride=2 * tiles)
            wide_ref[rows, :] = gates[:, cols]
            push_re_ref[rows, :] = pushes[0][:, cols]
            push_im_ref[rows, :] = pushes[1][:, cols]
            at = k * tiles + j
            step_ref[at : at + 1, :] = step_re[:, cols]
            step_ref[2 * tiles + at : 2 * tiles + at + 1, :] = step_im[:, cols]


def local_kernel(
    x_ref, gate_ref, rate_ref, turn_ref, drive_re_ref, drive_im_ref,
    send_ref, push_re_ref, push_im_ref, wide_ref, step_ref, pair_ref,
):
    pushed(
        x_ref, gate_ref, rate_ref, turn_ref, drive_re_ref, drive_im_ref,
        push_re_ref, push_im_ref, wide_ref, step_ref,
    )
    groups = rate_ref.shape[1]
    high = step_ref.shape[0] // 2
    tiles = high // 2
    half = x_ref.shape[0] // 2
    w = (step_ref[0:high, :], step_ref[high : 2 * high, :])

    def advance(t, carried):
        states = []
        for side, (re, im) in enumerate(carried[:2]):
            at = pl.ds(pl.multiple_of((t + side * half) * high, high), high)
            factor = wide_ref[at, :]
            a_re, a_im = factor * w[0], factor * w[1]
            states.append(
                (
                    (push_re_ref[at, :] + a_re * re) - a_im * im,
                    (push_im_ref[at, :] + a_re * im) + a_im * re,
                )
            )
        return (*states, cmul((a_re, a_im), carried[2]))

    zero, one = jnp.zeros((high, lanes), f32), jnp.ones((high, lanes), f32)
    early, late, faded = lax.fori_loop(
        0, half, advance, ((zero, zero), (zero, zero), (one, zero)), unroll=8
    )
    whole = cmul(faded, early)
    step_ref[0:high, :] = late[0] + whole[0]
    step_ref[high : 2 * high, :] = late[1] + whole[1]
    total = jnp.sum(gate_ref[...], axis=1, keepdims=True)
    thin = iota((groups, lanes), 0) == iota((groups, lanes), 1) // (lanes // groups)
    total = jnp.sum(jnp.where(thin, total, 0.0), axis=0, keepdims=True)
    total_high = total.astype(bf16).astype(f32)
    for k in range(2):
        for part, rest in enumerate((total_high, total - total_high)):
            at = 2 * k + part
            for j in range(tiles):
                row = part * high + k * tiles + j
                pair_ref[at : at + 1, j * lanes : (j + 1) * lanes] = step_ref[row : row + 1, :]
            pair_ref[at : at + 1, tiles * lanes :] = rest
    forward, backward = pair_ref[0:2, :], pair_ref[2:4, :]
    here = lax.axis_index("sp")
    for block in range(send_ref.shape[0]):
        send_ref[block] = jnp.where(block > here, forward, backward).astype(bf16)


def powers(step, length, backward):
    width = step[0].shape[1]
    exponent = iota((8, width), 0)
    exponent = 8 - exponent if backward else exponent + 1
    current = step
    rows = (jnp.ones((8, width), f32), jnp.zeros((8, width), f32))
    for bit in range(4):
        taken = (exponent >> bit) % 2 == 1
        more = cmul(rows, current)
        rows = tuple(jnp.where(taken, m, r) for m, r in zip(more, rows))
        if bit < 3:
            current = cmul(current, current)
    grown = {8: (rows, current)}
    size = 8
    while size * 2 <= length:
        rows, current = grown[size]
        more = cmul(rows, current)
        pair = (more, rows) if backward else (rows, more)
        rows = tuple(jnp.concatenate([a, b], axis=0) for a, b in zip(*pair))
        grown[size * 2] = (rows, cmul(current, current))
        size *= 2
    rows, current = grown[size]
    rest = length - size
    if rest:
        tail_rows, tail_power = grown[rest]
        more = cmul(tail_rows, current)
        pair = (more, rows) if backward else (rows, more)
        rows = tuple(jnp.concatenate([a, b], axis=0) for a, b in zip(*pair))
        current = cmul(current, tail_power)
    return rows, current


def powers_at(step, exponents, most):
    rows = (jnp.ones(exponents.shape, f32), jnp.zeros(exponents.shape, f32))
    bit = 0
    while (1 << bit) <= most:
        taken = (exponents >> bit) % 2 == 1
        more = cmul(rows, step)
        rows = tuple(jnp.where(taken, m, r) for m, r in zip(more, rows))
        step = cmul(step, step)
        bit += 1
    return rows


def beside_kernel(
    x_ref, gate_ref, rate_ref, turn_ref, drive_re_ref, drive_im_ref, read_re_ref, read_im_ref,
    skip_ref, routes_ref, group_ref, weight_ref,
    local_ref, chain_ref, pick_ref, mix_ref,
    state_re_ref, state_im_ref, wide_ref, step_ref,
):
    length = x_ref.shape[0]
    groups, states = rate_ref.shape[1:]
    width = groups * states
    tiles = width // lanes
    blocks = chain_ref.shape[1]
    here = lax.axis_index("sp")
    pushed(
        x_ref, gate_ref, rate_ref, turn_ref, drive_re_ref, drive_im_ref,
        state_re_ref, state_im_ref, wide_ref, step_ref,
    )
    high = 2 * tiles
    w_re = step_ref[0:high, :]
    w_im = step_ref[high : 2 * high, :]

    def advance(t, carried):
        re, im = carried
        at = pl.ds(pl.multiple_of(t * high, high), high)
        factor = wide_ref[at, :]
        a_re, a_im = factor * w_re, factor * w_im
        new_re = (state_re_ref[at, :] + a_re * re) - a_im * im
        new_im = (state_im_ref[at, :] + a_re * im) + a_im * re
        state_re_ref[at, :] = new_re
        state_im_ref[at, :] = new_im
        return new_re, new_im

    zero = jnp.zeros((high, lanes), f32)
    lax.fori_loop(0, length, advance, (zero, zero), unroll=8)
    rows, cols = iota((length, length), 0), iota((length, length), 1)
    outs, wholes = [], []
    for k in range(2):
        total = None
        for part, state_ref in enumerate((state_re_ref, state_im_ref)):
            read_ref = (read_re_ref, read_im_ref)[part]
            table_high, table_low = split(block_diagonal(read_ref[k], groups, states), 2)
            for j in range(tiles):
                state = state_ref[pl.ds(k * tiles + j, length, stride=2 * tiles), :]
                state_high, state_low = split(state, 2)
                lane = slice(j * lanes, (j + 1) * lanes)
                value = (
                    mm_nt(state_high, table_high[:, lane])
                    + mm_nt(state_low, table_high[:, lane])
                    + mm_nt(state_high, table_low[:, lane])
                )
                if part:
                    value = -value
                total = value if total is None else total + value
        outs.append(total)
        step = steps_of(rate_ref[k], turn_ref[k], groups, states)
        whole = powers_at(step, jnp.full((1, width), length, jnp.int32), length)
        wholes.append(whole)
    source = iota((blocks, width), 0)
    earlier = source < here
    gap = jnp.where(earlier, here - 1 - source, source - 1 - here)
    whole = tuple(jnp.where(earlier, a, b) for a, b in zip(*wholes))
    chained = powers_at(whole, jnp.maximum(gap, 0), blocks - 1)
    for part in range(2):
        chain_ref[part] = jnp.where(gap >= 0, chained[part], 0.0)
    local_ref[...] = (
        outs[0] + exact_left(reversal(length), outs[1]) + skip_ref[...] * x_ref[...].astype(f32)
    )
    slots, share = pick_ref.shape
    routes = routes_ref[...]
    weights = weight_ref[...]
    scaled = group_ref[...] * weights / (weights[0:1] + weights[1:2])
    place = iota((slots, length), 0)
    first = routes[0:1] == place // 2
    second = routes[1:2] == place // 2
    named = jnp.where(first | second, 1.0, 0.0)
    before = (rows < cols) & (rows // share == cols // share)
    prior = mm(named.astype(bf16), before.astype(f32).astype(bf16))
    picked = jnp.where(prior == (place % 2).astype(f32), named, 0.0)
    base = lax.axis_index("tp") * share
    own = (iota((length, share), 0) == base + iota((length, share), 1)).astype(f32).astype(bf16)
    pick_ref[...] = mm(picked.astype(bf16), own).astype(bf16)
    own = (iota((share, length), 1) == base + iota((share, length), 0)).astype(f32).astype(bf16)
    mixing = None
    for piece in split(picked * jnp.where(first, scaled[0:1], scaled[1:2]), 3):
        more = mm_nt(own, piece)
        mixing = more if mixing is None else mixing + more
    mix_ref[...] = mixing


def carry_kernel(
    come_ref, local_ref, gate_ref, chain_ref, rate_ref, turn_ref, read_re_ref, read_im_ref,
    own_ref, next_ref, last_ref, far_ref, act_ref, lines_ref,
):
    here, member = lax.axis_index("sp"), lax.axis_index("tp")
    blocks, width = chain_ref.shape[1:]
    groups, states = rate_ref.shape[1:]
    tiles = width // lanes
    length = local_ref.shape[0]
    for block in range(blocks):
        pair = come_ref[block].astype(f32)
        for j in range(tiles + 1):
            at = 2 * (j * blocks + block)
            lines_ref[at : at + 2, :] = pair[:, j * lanes : (j + 1) * lanes]

    def lines_of(part, j):
        return lines_ref[pl.ds(2 * j * blocks + part, blocks, stride=2), :]

    came = [
        jnp.concatenate([lines_of(part, j) for j in range(tiles)], axis=1) for part in range(2)
    ]
    logs = lines_of(0, tiles) + lines_of(1, tiles)
    each = lanes // groups
    fan = (iota((lanes, width), 0) == each * (iota((lanes, width), 1) // states)).astype(f32)
    fan = fan.astype(bf16)
    thin = (iota((groups, lanes), 0) == iota((groups, lanes), 1) // each).astype(f32).astype(bf16)
    source, mid = iota((blocks, blocks), 0), iota((blocks, blocks), 1)
    rows, cols = iota((length, length), 0), iota((length, length), 1)
    between = ((mid > source) & (mid < here)) | ((mid < source) & (mid > here))
    between = jnp.where(between & (source != here), 1.0, 0.0).astype(bf16)
    fade = exact_right(jnp.exp(exact_left(between, logs)), fan)
    gathered = cmul((chain_ref[0] * fade, chain_ref[1] * fade), came)
    earlier = iota((blocks, width), 0) < here
    total = local_ref[...]
    for k in range(2):
        taken = earlier if k == 0 else ~earlier
        carry = [jnp.sum(jnp.where(taken, v, 0.0), axis=0, keepdims=True) for v in gathered]
        real = block_diagonal(read_re_ref[k], groups, states)
        imaginary = block_diagonal(read_im_ref[k], groups, states)
        step = steps_of(rate_ref[k], turn_ref[k], groups, states)
        grown, _ = powers(step, length, k == 1)
        first = carry[0] * real - carry[1] * imaginary
        second = -(carry[0] * imaginary + carry[1] * real)
        value = None
        for part, side in enumerate((first, second)):
            side_high, side_low = split(side, 2)
            high, low = split(grown[part], 2)
            more = mm_nt(high, side_high) + mm_nt(low, side_high) + mm_nt(high, side_low)
            value = more if value is None else value + more
        seen = (rows <= cols) if k == 0 else (rows >= cols)
        fade = jnp.exp(exact_right(gate_ref[...], seen.astype(f32).astype(bf16)))
        run = None
        for piece in split(fade, 3):
            more = mm_tn(piece, thin)
            run = more if run is None else run + more
        total = total + run * value
    act_ref[...] = jax.nn.gelu(total).astype(bf16)
    share = own_ref.shape[0]
    members = act_ref.shape[0] // share
    for shift, out_ref in enumerate((own_ref, next_ref, far_ref, last_ref)):
        at = lax.rem(member + shift, members) * share
        out_ref[...] = act_ref[pl.ds(pl.multiple_of(at, share), share), :]


def normed(values, gain):
    center = values - jnp.mean(values, axis=-1, keepdims=True)
    spread = jnp.mean(center * center, axis=-1, keepdims=True)
    return center * lax.rsqrt(spread + norm_epsilon) * gain


def to_lines(rows, rows_ref, out_ref):
    count, width = rows.shape
    each = width // lanes
    for q in range(each):
        rows_ref[pl.ds(q, count, stride=each), :] = rows[:, q * lanes : (q + 1) * lanes]
    out_ref[...] = rows_ref[...].astype(bf16)


def from_lines(lines_ref, rows_ref, each):
    count = lines_ref.shape[0] // each
    rows_ref[...] = lines_ref[...].astype(f32)
    return [rows_ref[pl.ds(q, count, stride=each), :].astype(bf16) for q in range(each)]


def branch_kernel(
    own_ref, from_last_ref, from_far_ref, from_next_ref, weight_ref, residual_ref, gain_ref,
    pick_ref, middle_ref, out_ref, rows_ref,
):
    member = lax.axis_index("tp")
    channels = own_ref.shape[1]
    members = weight_ref.shape[0] // channels
    branch = None
    for shift, part_ref in enumerate((own_ref, from_next_ref, from_far_ref, from_last_ref)):
        at = lax.rem(member + shift, members) * channels
        more = mm(part_ref[...], weight_ref[pl.ds(pl.multiple_of(at, channels), channels), :])
        branch = more if branch is None else branch + more
    middle = normed(deep_alpha * residual_ref[...].astype(f32) + branch, gain_ref[...])
    middle_ref[...] = middle
    to_lines(mm(pick_ref[...], middle.astype(bf16)), rows_ref, out_ref)


def hidden_kernel(top_ref, low_ref, gate_ref, linear_ref, out_ref, rows_ref):
    each = gate_ref.shape[0] // lanes
    half = top_ref.shape[0] // each
    for at, ref in ((0, top_ref), (half, low_ref)):
        rows = jnp.concatenate(from_lines(ref, rows_ref, each), axis=1)
        gate = mm(rows, gate_ref[...])
        linear = mm(rows, linear_ref[...])
        out_ref[at : at + half, :] = (jax.nn.silu(gate) * linear).astype(bf16)


def down_kernel(own_ref, last_ref, next_ref, w_own_ref, w_last_ref, w_next_ref, out_ref):
    total = mm(own_ref[...], w_own_ref[...]).astype(bf16).astype(f32)
    total = total + mm(last_ref[...], w_last_ref[...]).astype(bf16).astype(f32)
    out_ref[...] = total + mm(next_ref[...], w_next_ref[...]).astype(bf16).astype(f32)


def answer_kernel(sum_ref, far_ref, w_far_top_ref, w_far_low_ref, out_ref, rows_ref):
    half = w_far_top_ref.shape[0]
    far = mm(far_ref[:, :half], w_far_top_ref[...]) + mm(far_ref[:, half:], w_far_low_ref[...])
    to_lines(sum_ref[...] + far.astype(bf16).astype(f32), rows_ref, out_ref)


def final_kernel(answers_ref, mix_ref, middle_ref, gain_ref, out_ref, rows_ref):
    each = middle_ref.shape[1] // lanes
    mixing = split(mix_ref[...], 3)
    routed = []
    for answers in from_lines(answers_ref, rows_ref, each):
        routed.append(mm(mixing[0], answers) + mm(mixing[1], answers) + mm(mixing[2], answers))
    routed = jnp.concatenate(routed, axis=1)
    out_ref[...] = normed(deep_alpha * middle_ref[...] + routed, gain_ref[...]).astype(bf16)


def shape(dims, dtype):
    return jax.ShapeDtypeStruct(dims, dtype)


def call(kernel, outs, scratch, cost, *args, room=16, kept=0):
    many = isinstance(outs, (list, tuple))
    whole = pl.BlockSpec(memory_space=VMEM)
    return pl.pallas_call(
        kernel,
        out_shape=outs,
        in_specs=[pl.BlockSpec(memory_space=pl.ANY)] * kept + [whole] * (len(args) - kept),
        out_specs=[whole] * len(outs) if many else whole,
        scratch_shapes=scratch,
        compiler_params=pltpu.CompilerParams(vmem_limit_bytes=room << 20),
        cost_estimate=pl.CostEstimate(flops=cost, bytes_accessed=1 << 20, transcendentals=0),
    )(*args)


def on_device(
    residual, mixer_input, log_gate, decay_rate, turn_rate, drive_real, drive_imaginary,
    read_real, read_imaginary, skip_gain, project_weight, norm_gain, final_gain, routes,
    group_weight, expert_weight, gate_weight, linear_weight, down_weight,
):
    length, channels = mixer_input.shape
    groups, states = decay_rate.shape[1:]
    width = groups * states
    share, model = residual.shape
    blocks = lax.axis_size("sp")
    members = lax.axis_size("tp")
    slots = 2 * blocks
    right = [(i, (i + 1) % members) for i in range(members)]
    left = [(i, (i - 1) % members) for i in range(members)]
    across = [(i, (i + 2) % members) for i in range(members)]

    def moved(array, way):
        return lax.ppermute(array, "tp", way)

    down = down_weight[0]
    half_down = down.shape[0] // 2
    down_last = moved(down, right)
    down_next = moved(down, left)

    flat = lambda table: table.reshape(2, -1, states)
    rows = length * 2 * width // lanes
    swept = [pltpu.VMEM((rows, lanes), f32)] * 3 + [pltpu.VMEM((4 * width // lanes, lanes), f32)]
    send = call(
        local_kernel, shape((blocks, 2, width + lanes), bf16),
        swept + [pltpu.VMEM((8, width + lanes), f32)], 1 << 30,
        mixer_input, log_gate.T, decay_rate, turn_rate, flat(drive_real), flat(drive_imaginary),
        room=60,
    )
    come = lax.all_to_all(send, "sp", split_axis=0, concat_axis=0, tiled=True)
    local, chain, pick, mix = call(
        beside_kernel,
        [
            shape((length, lanes), f32),
            shape((2, blocks, width), f32),
            shape((slots, share), bf16),
            shape((share, slots), f32),
        ],
        swept,
        1 << 30,
        mixer_input, log_gate.T, decay_rate, turn_rate, flat(drive_real),
        flat(drive_imaginary), flat(read_real), flat(read_imaginary), skip_gain[None], routes.T, group_weight[None], expert_weight.T,
        room=40,
    )
    own, to_next, to_last, to_far = call(
        carry_kernel,
        [shape((share, channels), bf16)] * 4,
        [
            pltpu.VMEM((length, channels), bf16),
            pltpu.VMEM((2 * blocks * (width // lanes + 1), lanes), f32),
        ],
        1 << 29,
        come, local, log_gate.T, chain, decay_rate, turn_rate, flat(read_real), flat(read_imaginary),
        room=40,
    )
    from_far = moved(to_far, across)
    from_last = moved(to_next, right)
    from_next = moved(to_last, left)
    down_far_top = moved(down_last[:half_down], right)
    down_far_low = moved(down_next[half_down:], left)
    lines = slots * model // lanes
    middle, outgoing = call(
        branch_kernel,
        [shape((share, model), f32), shape((lines, lanes), bf16)],
        [pltpu.VMEM((lines, lanes), f32)],
        1 << 29,
        own, from_last, from_far, from_next, project_weight, residual, norm_gain[None], pick,
    )

    def exchanged(array):
        return lax.all_to_all(
            array.reshape(blocks, lines // blocks, lanes), "sp", split_axis=0, concat_axis=0,
            tiled=True,
        ).reshape(lines, lanes)

    landed = exchanged(outgoing)
    top, low = landed[: lines // 2], landed[lines // 2 :]
    last_top = moved(top, right)
    next_low = moved(low, left)
    last_low = moved(low, right)
    next_top = moved(top, left)
    far_top = moved(last_top, right)
    far_low = moved(next_low, left)

    def hidden_of(upper, lower):
        return call(
            hidden_kernel, shape((slots, gate_weight.shape[2]), bf16),
            [pltpu.VMEM((lines // 2, lanes), f32)], 1 << 29,
            upper, lower, gate_weight[0], linear_weight[0],
        )

    hidden_own = hidden_of(top, low)
    hidden_last = moved(hidden_of(last_top, last_low), left)
    hidden_next = moved(hidden_of(next_top, next_low), right)
    hidden_far = moved(hidden_of(far_top, far_low), across)
    summed = call(
        down_kernel, shape((slots, model), f32), [], 1 << 29,
        hidden_own, hidden_next, hidden_last, down, down_last, down_next,
    )
    answers = call(
        answer_kernel, shape((lines, lanes), bf16), [pltpu.VMEM((lines, lanes), f32)], 1 << 28,
        summed, hidden_far, down_far_top, down_far_low,
    )
    returned = exchanged(answers)
    return call(
        final_kernel, shape((share, model), bf16), [pltpu.VMEM((lines, lanes), f32)], 1 << 28,
        returned, mix, middle, final_gain[None],
    )


def solution(mesh):
    placed = (
        P(("sp", "tp"), None), P("sp", "tp"), P("sp", "tp"),
        P(None, "tp", None), P(None, "tp", None),
        P(None, "tp", None, None), P(None, "tp", None, None),
        P(None, "tp", None, None), P(None, "tp", None, None),
        P("tp"), P(), P(), P(),
        P("sp", None), P("sp"), P("sp", None),
        P("sp", None, "tp"), P("sp", None, "tp"), P("sp", "tp", None),
    )

    return jax.shard_map(
        on_device, mesh=mesh, in_specs=placed, out_specs=P(("sp", "tp"), None), check_vma=False
    )
```

```python
import jax
import jax.numpy as jnp
from jax import lax
from jax.experimental import pallas as pl
from jax.experimental.pallas import tpu as pltpu
from jax.sharding import PartitionSpec as P


deep_alpha = 2.0**0.25
norm_epsilon = 1e-05
f32 = jnp.float32
bf16 = jnp.bfloat16
VMEM = pltpu.MemorySpace.VMEM
lanes = 128


def iota(shape, dim):
    return lax.broadcasted_iota(jnp.int32, shape, dim)


def mm(a, b):
    return lax.dot_general(a, b, (((1,), (0,)), ((), ())), preferred_element_type=f32)


def mm_nt(a, b):
    return lax.dot_general(a, b, (((1,), (1,)), ((), ())), preferred_element_type=f32)


def mm_tn(a, b):
    return lax.dot_general(a, b, (((0,), (0,)), ((), ())), preferred_element_type=f32)


def split(value, pieces):
    found = []
    for _ in range(pieces - 1):
        high = value.astype(bf16)
        found.append(high)
        value = value - high.astype(f32)
    return found + [value.astype(bf16)]


def exact_left(table, value):
    total = None
    for piece in split(value, 3):
        part = mm(table, piece)
        total = part if total is None else total + part
    return total


def exact_right(value, table):
    total = None
    for piece in split(value, 3):
        part = mm(piece, table)
        total = part if total is None else total + part
    return total


def reversal(size):
    return (iota((size, size), 0) + iota((size, size), 1) == size - 1).astype(f32).astype(bf16)


def as_row(table, groups, states):
    wide = jnp.concatenate([table] * groups, axis=1)
    keep = iota(wide.shape, 0) == iota(wide.shape, 1) // states
    return jnp.sum(jnp.where(keep, wide, 0.0), axis=0, keepdims=True)


def block_diagonal(table, groups, states):
    each = table.shape[0] // groups
    wide = jnp.concatenate([table] * groups, axis=1)
    keep = iota(wide.shape, 0) // each == iota(wide.shape, 1) // states
    return jnp.where(keep, wide, 0.0)


def steps_of(rate, turn, groups, states):
    retain = jnp.exp(-rate)
    return (
        as_row(retain * jnp.cos(turn), groups, states),
        as_row(retain * jnp.sin(turn), groups, states),
    )


def cmul(a, b):
    return (a[0] * b[0] - a[1] * b[1], a[0] * b[1] + a[1] * b[0])


def pushed(
    x_ref, gate_ref, rate_ref, turn_ref, drive_re_ref, drive_im_ref,
    push_re_ref, push_im_ref, wide_ref, step_ref,
):
    length = x_ref.shape[0]
    groups, states = rate_ref.shape[1:]
    width = groups * states
    tiles = width // lanes
    turned = reversal(length)
    x = x_ref[...]
    spread = (iota((groups, width), 0) == iota((groups, width), 1) // states).astype(f32).astype(bf16)
    factors = split(jnp.exp(gate_ref[...]), 3)
    for k in range(2):
        rate = rate_ref[k]
        step_re, step_im = steps_of(rate, turn_ref[k], groups, states)
        scale = as_row(jnp.sqrt(1.0 - jnp.exp(-2.0 * rate)), groups, states)
        x_k = x if k == 0 else mm(turned, x).astype(bf16)
        x_two = jnp.concatenate([x_k, x_k], axis=1)
        gates = None
        for piece in factors:
            piece_k = piece if k == 0 else mm(piece, turned).astype(bf16)
            part = mm_tn(piece_k, spread)
            gates = part if gates is None else gates + part
        pushes = []
        for drive_ref in (drive_re_ref, drive_im_ref):
            table = block_diagonal(drive_ref[k], groups, states) * scale
            pushes.append(mm(x_two, jnp.concatenate(split(table, 2), axis=0)))
        for j in range(tiles):
            cols = slice(j * lanes, (j + 1) * lanes)
            rows = pl.ds(k * tiles + j, length, stride=2 * tiles)
            wide_ref[rows, :] = gates[:, cols]
            push_re_ref[rows, :] = pushes[0][:, cols]
            push_im_ref[rows, :] = pushes[1][:, cols]
            at = k * tiles + j
            step_ref[at : at + 1, :] = step_re[:, cols]
            step_ref[2 * tiles + at : 2 * tiles + at + 1, :] = step_im[:, cols]


def local_kernel(
    x_ref, gate_ref, rate_ref, turn_ref, drive_re_ref, drive_im_ref,
    send_ref, push_re_ref, push_im_ref, wide_ref, step_ref, pair_ref,
):
    pushed(
        x_ref, gate_ref, rate_ref, turn_ref, drive_re_ref, drive_im_ref,
        push_re_ref, push_im_ref, wide_ref, step_ref,
    )
    groups = rate_ref.shape[1]
    high = step_ref.shape[0] // 2
    tiles = high // 2
    parts = 4
    span = x_ref.shape[0] // parts
    w = (step_ref[0:high, :], step_ref[high : 2 * high, :])

    def advance(t, carried):
        states, faded = carried
        new_states, new_faded = [], []
        for side, (re, im) in enumerate(states):
            at = pl.ds(pl.multiple_of((t + side * span) * high, high), high)
            factor = wide_ref[at, :]
            a_re, a_im = factor * w[0], factor * w[1]
            new_states.append(
                (
                    (push_re_ref[at, :] + a_re * re) - a_im * im,
                    (push_im_ref[at, :] + a_re * im) + a_im * re,
                )
            )
            if side:
                new_faded.append(cmul((a_re, a_im), faded[side - 1]))
        return tuple(new_states), tuple(new_faded)

    zero, one = jnp.zeros((high, lanes), f32), jnp.ones((high, lanes), f32)
    states, faded = lax.fori_loop(
        0, span, advance, (((zero, zero),) * parts, ((one, zero),) * (parts - 1)), unroll=4
    )
    last = states[0]
    for state, fade in zip(states[1:], faded):
        last = tuple(s + f for s, f in zip(state, cmul(fade, last)))
    step_ref[0:high, :] = last[0]
    step_ref[high : 2 * high, :] = last[1]
    total = jnp.sum(gate_ref[...], axis=1, keepdims=True)
    thin = iota((groups, lanes), 0) == iota((groups, lanes), 1) // (lanes // groups)
    total = jnp.sum(jnp.where(thin, total, 0.0), axis=0, keepdims=True)
    total_high = total.astype(bf16).astype(f32)
    for k in range(2):
        for part, rest in enumerate((total_high, total - total_high)):
            at = 2 * k + part
            for j in range(tiles):
                row = part * high + k * tiles + j
                pair_ref[at : at + 1, j * lanes : (j + 1) * lanes] = step_ref[row : row + 1, :]
            pair_ref[at : at + 1, tiles * lanes :] = rest
    forward, backward = pair_ref[0:2, :], pair_ref[2:4, :]
    here = lax.axis_index("sp")
    for block in range(send_ref.shape[0]):
        send_ref[block] = jnp.where(block > here, forward, backward).astype(bf16)


def powers(step, length, backward):
    width = step[0].shape[1]
    exponent = iota((8, width), 0)
    exponent = 8 - exponent if backward else exponent + 1
    current = step
    rows = (jnp.ones((8, width), f32), jnp.zeros((8, width), f32))
    for bit in range(4):
        taken = (exponent >> bit) % 2 == 1
        more = cmul(rows, current)
        rows = tuple(jnp.where(taken, m, r) for m, r in zip(more, rows))
        if bit < 3:
            current = cmul(current, current)
    grown = {8: (rows, current)}
    size = 8
    while size * 2 <= length:
        rows, current = grown[size]
        more = cmul(rows, current)
        pair = (more, rows) if backward else (rows, more)
        rows = tuple(jnp.concatenate([a, b], axis=0) for a, b in zip(*pair))
        grown[size * 2] = (rows, cmul(current, current))
        size *= 2
    rows, current = grown[size]
    rest = length - size
    if rest:
        tail_rows, tail_power = grown[rest]
        more = cmul(tail_rows, current)
        pair = (more, rows) if backward else (rows, more)
        rows = tuple(jnp.concatenate([a, b], axis=0) for a, b in zip(*pair))
        current = cmul(current, tail_power)
    return rows, current


def powers_at(step, exponents, most):
    rows = (jnp.ones(exponents.shape, f32), jnp.zeros(exponents.shape, f32))
    bit = 0
    while (1 << bit) <= most:
        taken = (exponents >> bit) % 2 == 1
        more = cmul(rows, step)
        rows = tuple(jnp.where(taken, m, r) for m, r in zip(more, rows))
        step = cmul(step, step)
        bit += 1
    return rows


def beside_kernel(
    x_ref, gate_ref, rate_ref, turn_ref, drive_re_ref, drive_im_ref, read_re_ref, read_im_ref,
    skip_ref, routes_ref, group_ref, weight_ref,
    local_ref, chain_ref, pick_ref, mix_ref,
    state_re_ref, state_im_ref, wide_ref, step_ref,
):
    length = x_ref.shape[0]
    groups, states = rate_ref.shape[1:]
    width = groups * states
    tiles = width // lanes
    blocks = chain_ref.shape[1]
    here = lax.axis_index("sp")
    pushed(
        x_ref, gate_ref, rate_ref, turn_ref, drive_re_ref, drive_im_ref,
        state_re_ref, state_im_ref, wide_ref, step_ref,
    )
    high = 2 * tiles
    w_re = step_ref[0:high, :]
    w_im = step_ref[high : 2 * high, :]

    def advance(t, carried):
        re, im = carried
        at = pl.ds(pl.multiple_of(t * high, high), high)
        factor = wide_ref[at, :]
        a_re, a_im = factor * w_re, factor * w_im
        new_re = (state_re_ref[at, :] + a_re * re) - a_im * im
        new_im = (state_im_ref[at, :] + a_re * im) + a_im * re
        state_re_ref[at, :] = new_re
        state_im_ref[at, :] = new_im
        return new_re, new_im

    zero = jnp.zeros((high, lanes), f32)
    lax.fori_loop(0, length, advance, (zero, zero), unroll=8)
    rows, cols = iota((length, length), 0), iota((length, length), 1)
    outs, wholes = [], []
    for k in range(2):
        total = None
        for part, state_ref in enumerate((state_re_ref, state_im_ref)):
            read_ref = (read_re_ref, read_im_ref)[part]
            table_high, table_low = split(block_diagonal(read_ref[k], groups, states), 2)
            for j in range(tiles):
                state = state_ref[pl.ds(k * tiles + j, length, stride=2 * tiles), :]
                state_high, state_low = split(state, 2)
                lane = slice(j * lanes, (j + 1) * lanes)
                value = (
                    mm_nt(state_high, table_high[:, lane])
                    + mm_nt(state_low, table_high[:, lane])
                    + mm_nt(state_high, table_low[:, lane])
                )
                if part:
                    value = -value
                total = value if total is None else total + value
        outs.append(total)
        step = steps_of(rate_ref[k], turn_ref[k], groups, states)
        whole = powers_at(step, jnp.full((1, width), length, jnp.int32), length)
        wholes.append(whole)
    source = iota((blocks, width), 0)
    earlier = source < here
    gap = jnp.where(earlier, here - 1 - source, source - 1 - here)
    whole = tuple(jnp.where(earlier, a, b) for a, b in zip(*wholes))
    chained = powers_at(whole, jnp.maximum(gap, 0), blocks - 1)
    for part in range(2):
        chain_ref[part] = jnp.where(gap >= 0, chained[part], 0.0)
    local_ref[...] = (
        outs[0] + exact_left(reversal(length), outs[1]) + skip_ref[...] * x_ref[...].astype(f32)
    )
    slots, share = pick_ref.shape
    routes = routes_ref[...]
    weights = weight_ref[...]
    scaled = group_ref[...] * weights / (weights[0:1] + weights[1:2])
    place = iota((slots, length), 0)
    first = routes[0:1] == place // 2
    second = routes[1:2] == place // 2
    named = jnp.where(first | second, 1.0, 0.0)
    before = (rows < cols) & (rows // share == cols // share)
    prior = mm(named.astype(bf16), before.astype(f32).astype(bf16))
    picked = jnp.where(prior == (place % 2).astype(f32), named, 0.0)
    base = lax.axis_index("tp") * share
    own = (iota((length, share), 0) == base + iota((length, share), 1)).astype(f32).astype(bf16)
    pick_ref[...] = mm(picked.astype(bf16), own).astype(bf16)
    own = (iota((share, length), 1) == base + iota((share, length), 0)).astype(f32).astype(bf16)
    mixing = None
    for piece in split(picked * jnp.where(first, scaled[0:1], scaled[1:2]), 3):
        more = mm_nt(own, piece)
        mixing = more if mixing is None else mixing + more
    mix_ref[...] = mixing


def carry_kernel(
    come_ref, local_ref, gate_ref, chain_ref, rate_ref, turn_ref, read_re_ref, read_im_ref,
    own_ref, next_ref, last_ref, far_ref, act_ref, lines_ref,
):
    here, member = lax.axis_index("sp"), lax.axis_index("tp")
    blocks, width = chain_ref.shape[1:]
    groups, states = rate_ref.shape[1:]
    tiles = width // lanes
    length = local_ref.shape[0]
    for block in range(blocks):
        pair = come_ref[block].astype(f32)
        for j in range(tiles + 1):
            at = 2 * (j * blocks + block)
            lines_ref[at : at + 2, :] = pair[:, j * lanes : (j + 1) * lanes]

    def lines_of(part, j):
        return lines_ref[pl.ds(2 * j * blocks + part, blocks, stride=2), :]

    came = [
        jnp.concatenate([lines_of(part, j) for j in range(tiles)], axis=1) for part in range(2)
    ]
    logs = lines_of(0, tiles) + lines_of(1, tiles)
    each = lanes // groups
    fan = (iota((lanes, width), 0) == each * (iota((lanes, width), 1) // states)).astype(f32)
    fan = fan.astype(bf16)
    thin = (iota((groups, lanes), 0) == iota((groups, lanes), 1) // each).astype(f32).astype(bf16)
    source, mid = iota((blocks, blocks), 0), iota((blocks, blocks), 1)
    rows, cols = iota((length, length), 0), iota((length, length), 1)
    between = ((mid > source) & (mid < here)) | ((mid < source) & (mid > here))
    between = jnp.where(between & (source != here), 1.0, 0.0).astype(bf16)
    fade = exact_right(jnp.exp(exact_left(between, logs)), fan)
    gathered = cmul((chain_ref[0] * fade, chain_ref[1] * fade), came)
    earlier = iota((blocks, width), 0) < here
    total = local_ref[...]
    for k in range(2):
        taken = earlier if k == 0 else ~earlier
        carry = [jnp.sum(jnp.where(taken, v, 0.0), axis=0, keepdims=True) for v in gathered]
        real = block_diagonal(read_re_ref[k], groups, states)
        imaginary = block_diagonal(read_im_ref[k], groups, states)
        step = steps_of(rate_ref[k], turn_ref[k], groups, states)
        grown, _ = powers(step, length, k == 1)
        first = carry[0] * real - carry[1] * imaginary
        second = -(carry[0] * imaginary + carry[1] * real)
        value = None
        for part, side in enumerate((first, second)):
            side_high, side_low = split(side, 2)
            high, low = split(grown[part], 2)
            two = mm_nt(jnp.concatenate([high, low], axis=0), side_high)
            more = two[:length] + two[length:] + mm_nt(high, side_low)
            value = more if value is None else value + more
        seen = (rows <= cols) if k == 0 else (rows >= cols)
        fade = jnp.exp(exact_right(gate_ref[...], seen.astype(f32).astype(bf16)))
        run = None
        for piece in split(fade, 3):
            more = mm_tn(piece, thin)
            run = more if run is None else run + more
        total = total + run * value
    act_ref[...] = jax.nn.gelu(total).astype(bf16)
    share = own_ref.shape[0]
    members = act_ref.shape[0] // share
    for shift, out_ref in enumerate((own_ref, next_ref, far_ref, last_ref)):
        at = lax.rem(member + shift, members) * share
        out_ref[...] = act_ref[pl.ds(pl.multiple_of(at, share), share), :]


def normed(values, gain):
    center = values - jnp.mean(values, axis=-1, keepdims=True)
    spread = jnp.mean(center * center, axis=-1, keepdims=True)
    return center * lax.rsqrt(spread + norm_epsilon) * gain


def to_lines(rows, rows_ref, out_ref):
    count, width = rows.shape
    each = width // lanes
    for q in range(each):
        rows_ref[pl.ds(q, count, stride=each), :] = rows[:, q * lanes : (q + 1) * lanes]
    out_ref[...] = rows_ref[...].astype(bf16)


def from_lines(lines_ref, rows_ref, each):
    count = lines_ref.shape[0] // each
    rows_ref[...] = lines_ref[...].astype(f32)
    return [rows_ref[pl.ds(q, count, stride=each), :].astype(bf16) for q in range(each)]


def branch_kernel(
    own_ref, from_last_ref, from_far_ref, from_next_ref, weight_ref, residual_ref, gain_ref,
    pick_ref, middle_ref, out_ref, rows_ref,
):
    member = lax.axis_index("tp")
    channels = own_ref.shape[1]
    members = weight_ref.shape[0] // channels
    branch = None
    for shift, part_ref in enumerate((own_ref, from_next_ref, from_far_ref, from_last_ref)):
        at = lax.rem(member + shift, members) * channels
        more = mm(part_ref[...], weight_ref[pl.ds(pl.multiple_of(at, channels), channels), :])
        branch = more if branch is None else branch + more
    middle = normed(deep_alpha * residual_ref[...].astype(f32) + branch, gain_ref[...])
    middle_ref[...] = middle
    to_lines(mm(pick_ref[...], middle.astype(bf16)), rows_ref, out_ref)


def hidden_kernel(top_ref, low_ref, gate_ref, linear_ref, out_ref, top_rows, low_rows):
    each = gate_ref.shape[0] // lanes
    rows = jnp.concatenate(
        [
            jnp.concatenate(from_lines(ref, rows_ref, each), axis=1)
            for ref, rows_ref in ((top_ref, top_rows), (low_ref, low_rows))
        ],
        axis=0,
    )
    gate = mm(rows, gate_ref[...])
    linear = mm(rows, linear_ref[...])
    out_ref[...] = (jax.nn.silu(gate) * linear).astype(bf16)


def down_kernel(own_ref, last_ref, next_ref, w_own_ref, w_last_ref, w_next_ref, out_ref):
    total = mm(own_ref[...], w_own_ref[...]).astype(bf16).astype(f32)
    total = total + mm(last_ref[...], w_last_ref[...]).astype(bf16).astype(f32)
    out_ref[...] = total + mm(next_ref[...], w_next_ref[...]).astype(bf16).astype(f32)


def answer_kernel(sum_ref, far_ref, w_far_top_ref, w_far_low_ref, out_ref, rows_ref):
    half = w_far_top_ref.shape[0]
    far = mm(far_ref[:, :half], w_far_top_ref[...]) + mm(far_ref[:, half:], w_far_low_ref[...])
    to_lines(sum_ref[...] + far.astype(bf16).astype(f32), rows_ref, out_ref)


def final_kernel(answers_ref, mix_ref, middle_ref, gain_ref, out_ref, rows_ref):
    share, width = middle_ref.shape
    mixing = jnp.concatenate(split(mix_ref[...], 3), axis=0)
    routed = []
    for answers in from_lines(answers_ref, rows_ref, width // lanes):
        three = mm(mixing, answers)
        routed.append(three[:share] + three[share : 2 * share] + three[2 * share :])
    routed = jnp.concatenate(routed, axis=1)
    out_ref[...] = normed(deep_alpha * middle_ref[...] + routed, gain_ref[...]).astype(bf16)


def shape(dims, dtype):
    return jax.ShapeDtypeStruct(dims, dtype)


def call(kernel, outs, scratch, cost, *args, room=16, kept=0):
    many = isinstance(outs, (list, tuple))
    whole = pl.BlockSpec(memory_space=VMEM)
    return pl.pallas_call(
        kernel,
        out_shape=outs,
        in_specs=[pl.BlockSpec(memory_space=pl.ANY)] * kept + [whole] * (len(args) - kept),
        out_specs=[whole] * len(outs) if many else whole,
        scratch_shapes=scratch,
        compiler_params=pltpu.CompilerParams(vmem_limit_bytes=room << 20),
        cost_estimate=pl.CostEstimate(flops=cost, bytes_accessed=1 << 20, transcendentals=0),
    )(*args)


def on_device(
    residual, mixer_input, log_gate, decay_rate, turn_rate, drive_real, drive_imaginary,
    read_real, read_imaginary, skip_gain, project_weight, norm_gain, final_gain, routes,
    group_weight, expert_weight, gate_weight, linear_weight, down_weight,
):
    length, channels = mixer_input.shape
    groups, states = decay_rate.shape[1:]
    width = groups * states
    share, model = residual.shape
    blocks = lax.axis_size("sp")
    members = lax.axis_size("tp")
    slots = 2 * blocks
    right = [(i, (i + 1) % members) for i in range(members)]
    left = [(i, (i - 1) % members) for i in range(members)]
    across = [(i, (i + 2) % members) for i in range(members)]

    def moved(array, way):
        return lax.ppermute(array, "tp", way)

    down = down_weight[0]
    half_down = down.shape[0] // 2
    down_last = moved(down, right)
    down_next = moved(down, left)

    flat = lambda table: table.reshape(2, -1, states)
    rows = length * 2 * width // lanes
    swept = [pltpu.VMEM((rows, lanes), f32)] * 3 + [pltpu.VMEM((4 * width // lanes, lanes), f32)]
    send = call(
        local_kernel, shape((blocks, 2, width + lanes), bf16),
        swept + [pltpu.VMEM((8, width + lanes), f32)], 1 << 30,
        mixer_input, log_gate.T, decay_rate, turn_rate, flat(drive_real), flat(drive_imaginary),
        room=60,
    )
    come = lax.all_to_all(send, "sp", split_axis=0, concat_axis=0, tiled=True)
    local, chain, pick, mix = call(
        beside_kernel,
        [
            shape((length, lanes), f32),
            shape((2, blocks, width), f32),
            shape((slots, share), bf16),
            shape((share, slots), f32),
        ],
        swept,
        1 << 30,
        mixer_input, log_gate.T, decay_rate, turn_rate, flat(drive_real),
        flat(drive_imaginary), flat(read_real), flat(read_imaginary), skip_gain[None], routes.T, group_weight[None], expert_weight.T,
        room=40,
    )
    own, to_next, to_last, to_far = call(
        carry_kernel,
        [shape((share, channels), bf16)] * 4,
        [
            pltpu.VMEM((length, channels), bf16),
            pltpu.VMEM((2 * blocks * (width // lanes + 1), lanes), f32),
        ],
        1 << 29,
        come, local, log_gate.T, chain, decay_rate, turn_rate, flat(read_real), flat(read_imaginary),
        room=40,
    )
    from_far = moved(to_far, across)
    from_last = moved(to_next, right)
    from_next = moved(to_last, left)
    down_far_top = moved(down_last[:half_down], right)
    down_far_low = moved(down_next[half_down:], left)
    lines = slots * model // lanes
    middle, outgoing = call(
        branch_kernel,
        [shape((share, model), f32), shape((lines, lanes), bf16)],
        [pltpu.VMEM((lines, lanes), f32)],
        1 << 29,
        own, from_last, from_far, from_next, project_weight, residual, norm_gain[None], pick,
    )

    def exchanged(array):
        return lax.all_to_all(
            array.reshape(blocks, lines // blocks, lanes), "sp", split_axis=0, concat_axis=0,
            tiled=True,
        ).reshape(lines, lanes)

    landed = exchanged(outgoing)
    top, low = landed[: lines // 2], landed[lines // 2 :]
    last_top = moved(top, right)
    next_low = moved(low, left)
    last_low = moved(low, right)
    next_top = moved(top, left)
    far_top = moved(last_top, right)
    far_low = moved(next_low, left)

    def hidden_of(upper, lower):
        return call(
            hidden_kernel, shape((slots, gate_weight.shape[2]), bf16),
            [pltpu.VMEM((lines // 2, lanes), f32)] * 2, 1 << 29,
            upper, lower, gate_weight[0], linear_weight[0],
        )

    hidden_own = hidden_of(top, low)
    hidden_last = moved(hidden_of(last_top, last_low), left)
    hidden_next = moved(hidden_of(next_top, next_low), right)
    hidden_far = moved(hidden_of(far_top, far_low), across)
    summed = call(
        down_kernel, shape((slots, model), f32), [], 1 << 29,
        hidden_own, hidden_next, hidden_last, down, down_last, down_next,
    )
    answers = call(
        answer_kernel, shape((lines, lanes), bf16), [pltpu.VMEM((lines, lanes), f32)], 1 << 28,
        summed, hidden_far, down_far_top, down_far_low,
    )
    returned = exchanged(answers)
    return call(
        final_kernel, shape((share, model), bf16), [pltpu.VMEM((lines, lanes), f32)], 1 << 28,
        returned, mix, middle, final_gain[None],
    )


def solution(mesh):
    placed = (
        P(("sp", "tp"), None), P("sp", "tp"), P("sp", "tp"),
        P(None, "tp", None), P(None, "tp", None),
        P(None, "tp", None, None), P(None, "tp", None, None),
        P(None, "tp", None, None), P(None, "tp", None, None),
        P("tp"), P(), P(), P(),
        P("sp", None), P("sp"), P("sp", None),
        P("sp", None, "tp"), P("sp", None, "tp"), P("sp", "tp", None),
    )

    return jax.shard_map(
        on_device, mesh=mesh, in_specs=placed, out_specs=P(("sp", "tp"), None), check_vma=False
    )
```
